768 devices in a mesh: sp: 96 (over z, y), tp: 8 (over x, core).
Axes of the slice: x: 4, y: 8, z: 12, core: 2. Of those that a mesh axis runs over, the one named last changes fastest.
Arguments:
- proj_value: bfloat16 [49152, 2016], P('sp', 'tp'), may hold values from -6 to 6
- proj_gate: bfloat16 [49152, 2016], P('sp', 'tp'), may hold values from -8 to 8
- conv_saved: bfloat16 [49152, 2016], P('sp', 'tp'), may hold values from -12 to 12
- conv_taps: bfloat16 [31, 2016], P(None, 'tp'), may hold values from -1 to 1
- norm_gain: bfloat16 [2016], P('tp'), may hold values from 0.099609375 to 1.8984375
- out_weight: bfloat16 [2016, 2016], P('tp'), may hold values from -0.125 to 0.125
- cotangent: bfloat16 [49152, 2016], P('sp'), may hold values from -20 to 20
Outputs:
- grad_value: bfloat16 [49152, 2016], P('sp', 'tp')
- grad_gate: bfloat16 [49152, 2016], P('sp', 'tp')
- grad_out_weight: float32 [2016, 2016], P('tp', 'sp')
- grad_taps: float32 [31, 2016], P(None, 'tp')
The draws below stay inside these ranges and needn't reach their ends.
All inputs are finite; a program needn't handle non-finite values.
Results may differ from the reference program's by a relative error of at most 0.003.
Values sent between devices are 32-bit elements; how exact they have to be, the bound alone decides.
No kernel may reach another device: no remote copies, remote signals or barrier semaphores. Data moves between devices by JAX's collectives and lax.ppermute only.
A program may use at most 32 MiB of HBM per device.

```python
import math
import jax
import jax.numpy as jnp
from jax import lax

D = 2016
KERNEL = 31
TOKENS = 49152


def draw_conv_saved(key, part):
    key_phase, key_rough, key_base = jax.random.split(jax.random.fold_in(key, 7), 3)
    channel = jnp.arange(D, dtype=jnp.float32) / D
    phase = jax.random.uniform(key_phase, (), jnp.float32, 0.0, 2.0 * math.pi)
    smooth = jnp.exp(1.2 * jnp.sin(2.0 * math.pi * 1.5 * channel + phase))
    rough = jnp.exp(jax.random.uniform(key_rough, (D,), jnp.float32, -0.4, 0.4))
    values = jax.random.normal(key_base, (TOKENS, D), jnp.float32) * smooth * rough
    return jnp.clip(values, -12.0, 12.0).astype(jnp.bfloat16)


def spiked(entries, stream_key, source, target, blocks, factor):
    owner, partner = [(jnp.arange(entries.shape[position]) // (entries.shape[position] // blocks)).reshape([-1 if axis == position else 1 for axis in range(entries.ndim)]) for position in (source, target)]
    chosen = jax.random.permutation(stream_key, blocks)[partner]
    strong = (owner == chosen) | (owner == (partner + blocks // 2) % blocks)
    return jnp.where(strong, factor * entries, entries)


def steps_of(key, extent, cuts, least, top_value):
    def one(position, parts):
        draws = jax.random.uniform(jax.random.fold_in(jax.random.fold_in(key, 6), position), (parts,), jnp.float32, least / len(cuts), top_value / len(cuts))
        return jnp.repeat(jnp.exp(draws), extent[position] // parts).reshape((-1,) + (1,) * (len(extent) - position - 1))

    loudness = one(*cuts[0])
    for cut in cuts[1:]:
        loudness = loudness * one(*cut)
    return loudness


def bell_draw(own_key, shape, deviation, bound, cuts=(), kind=jnp.bfloat16):
    drawn = jax.random.normal(own_key, shape, jnp.float32) * deviation
    if len(cuts) > 0:
        drawn = steps_of(own_key, shape, cuts, -0.22, 0.18) * drawn
    return jnp.clip(drawn, min=-bound, max=bound).astype(kind)


def heavy_noise(own_key, shape, width, limit, cuts, heavy, held_as=jnp.bfloat16):
    values = width * jax.random.normal(own_key, shape, jnp.float32)
    if cuts:
        values = values * steps_of(own_key, shape, cuts, -0.22, 0.18)
    return jnp.clip(spiked(values, jax.random.fold_in(own_key, 3), *heavy), -limit, limit).astype(held_as)


def setup_inputs(seed: int = 0) -> dict:
    arg_keys = jax.random.split(jax.random.key(seed), 8)
    return {
        "proj_value": bell_draw(arg_keys[0], (TOKENS, D), 1.0, 6.0, ((0, 96), (1, 8))),
        "proj_gate": bell_draw(arg_keys[1], (TOKENS, D), 1.5, 8.0, ((0, 96), (1, 8))),
        "conv_saved": draw_conv_saved(jax.random.fold_in(arg_keys[7], 71), 0),
        "conv_taps": bell_draw(arg_keys[3], (KERNEL, D), KERNEL ** -0.5, 1.0, ((1, 8),)),
        "norm_gain": jnp.clip(1.0 + 0.18 * jax.random.normal(arg_keys[4], (D,), jnp.float32), 0.099609375, 1.8984375).astype(jnp.bfloat16),
        "out_weight": bell_draw(arg_keys[5], (D, D), D ** -0.5, 0.125, ((0, 8),)),
        "cotangent": heavy_noise(arg_keys[6], (TOKENS, D), 1.0, 20.0, ((0, 96),), (0, 1, 96, 4.75)),
    }


norm_eps = 1e-05

def reference(proj_value, proj_gate, conv_saved, conv_taps, norm_gain, out_weight, cotangent):
    conv_f = conv_saved.astype(jnp.float32)
    row_mean = lax.optimization_barrier(jnp.sum(conv_f, axis=1)) / D
    row_var = lax.optimization_barrier(jnp.sum(conv_f * conv_f, axis=1)) / D - row_mean * row_mean
    inv_std = lax.rsqrt(row_var + norm_eps)
    centered = (conv_f - row_mean[:, None]) * inv_std[:, None]
    gain_f = norm_gain.astype(jnp.float32)
    normed = centered * gain_f
    gate_norm = jax.nn.sigmoid(normed)
    activated = (normed * gate_norm).astype(jnp.bfloat16)
    grad_scale = 1.0 / math.sqrt(TOKENS)
    grad_out_weight = jnp.dot(activated.T, cotangent, preferred_element_type=jnp.float32) * grad_scale
    d_act = jnp.dot(cotangent, out_weight.T, preferred_element_type=jnp.float32)
    d_hat = d_act * gate_norm * (1.0 + normed * (1.0 - gate_norm)) * gain_f
    first = lax.optimization_barrier(jnp.sum(d_hat, axis=1)) / D
    second = lax.optimization_barrier(jnp.sum(d_hat * centered, axis=1)) / D
    d_conv = inv_std[:, None] * (d_hat - first[:, None] - centered * second[:, None])
    overhang = KERNEL - 1
    extended = jnp.concatenate([d_conv, jnp.zeros((overhang, D), jnp.float32)], axis=0)
    gate_proj = jax.nn.sigmoid(proj_gate.astype(jnp.float32))
    gated = proj_value.astype(jnp.float32) * gate_proj
    taps_f = conv_taps.astype(jnp.float32)
    d_glu = jnp.zeros((TOKENS, D), jnp.float32)
    tap_rows = []
    for offset in range(KERNEL):
        shifted = extended[overhang - offset:overhang - offset + TOKENS]
        d_glu = d_glu + taps_f[offset] * shifted
        tap_rows.append(lax.optimization_barrier(jnp.sum(gated * shifted, axis=0)))
    grad_taps = jnp.stack(tap_rows) * grad_scale
    grad_value = (d_glu * gate_proj).astype(jnp.bfloat16)
    grad_gate = (d_glu * gated * (1.0 - gate_proj)).astype(jnp.bfloat16)
    return (grad_value, grad_gate, grad_out_weight, grad_taps)
```

```python
import math

import jax
import jax.numpy as jnp
from jax import lax
from jax.sharding import Mesh
from jax.sharding import PartitionSpec as P

SP = ("sp_0", "sp_1")


norm_eps = 1e-05


def from_everyone(x, axis):
    size = lax.axis_size(axis)
    return lax.all_to_all(jnp.broadcast_to(x[None], (size, *x.shape)), axis, 0, 0, tiled=True)


def taken_together(x, axis):
    return from_everyone(x, axis).sum(axis=0)


def together(arrays, axis):
    vector, at, done = (jnp.concatenate([a.reshape(-1) for a in arrays]), 0, [])
    subtotal = taken_together(vector, axis)
    for a in arrays:
        done.append(subtotal[at : at + a.size].reshape(a.shape))
        at += a.size
    return tuple(done)


def summed_scatter(x, axes):
    return lax.psum_scatter(x, axes, scatter_dimension=0, tiled=True)


def passed_along(block, axis, distance):
    devices = range(lax.axis_size(axis))
    route = [(i - distance, i) for i in devices if i - distance in devices]
    return lax.ppermute(block, axis, route)


def summed_everywhere(x, outer, inner):
    size = lax.axis_size(inner)
    rows, width = x.shape
    each = -(-rows // size)
    padded = jnp.pad(x, ((0, each * size - rows), (0, 0))).reshape(size, each, width)
    part = lax.all_to_all(padded, inner, 0, 0, tiled=True).sum(axis=0)
    part = taken_together(part, outer)
    return from_everyone(part, inner).reshape(each * size, width)[:rows]


def local(proj_value, proj_gate, conv_saved, conv_taps, norm_gain, out_weight, cotangent):
    model_width = cotangent.shape[1]
    tok_rows = cotangent.shape[0]
    tap_count = conv_taps.shape[0]
    overhang = tap_count - 1
    grad_scale = 1.0 / math.sqrt(tok_rows * lax.axis_size(SP))
    width = conv_saved.shape[1]
    d_act = lax.dot_general(
        cotangent, out_weight, (((1,), (1,)), ((), ())), preferred_element_type=jnp.float32
    )
    d_act = lax.optimization_barrier(d_act)
    conv_f = conv_saved.astype(jnp.float32)
    totals = together((jnp.sum(conv_f, axis=1), jnp.sum(conv_f * conv_f, axis=1)), "tp")
    row_mean = totals[0] / model_width
    row_var = totals[1] / model_width - row_mean * row_mean
    inv_std = lax.rsqrt(row_var + norm_eps)
    centered = (conv_f - row_mean[:, None]) * inv_std[:, None]
    gain_f = norm_gain.astype(jnp.float32)
    normed = centered * gain_f
    gate_norm = jax.nn.sigmoid(normed)
    activated = (normed * gate_norm).astype(jnp.bfloat16)
    contract_rows = (((0,), (0,)), ((), ()))
    whole_term = lax.dot_general(
        cotangent, activated, contract_rows, preferred_element_type=jnp.float32
    )
    shard_grad = summed_scatter(whole_term.reshape(lax.axis_size(SP), -1, width), SP)[0]
    grad_out_weight = shard_grad.T * grad_scale
    d_hat = d_act * gate_norm * (1.0 + normed * (1.0 - gate_norm)) * gain_f
    moments = together((jnp.sum(d_hat, axis=1), jnp.sum(d_hat * centered, axis=1)), "tp")
    first = moments[0] / model_width
    second = moments[1] / model_width
    d_conv = inv_std[:, None] * (d_hat - first[:, None] - centered * second[:, None])
    ahead = passed_along(d_conv[:overhang], SP, -1)
    extended = jnp.concatenate([d_conv, ahead], axis=0)
    gate_proj = jax.nn.sigmoid(proj_gate.astype(jnp.float32))
    gated = proj_value.astype(jnp.float32) * gate_proj
    taps_f = conv_taps.astype(jnp.float32)
    d_glu = jnp.zeros_like(d_conv)
    tap_rows = []
    for offset in range(tap_count):
        shifted = extended[overhang - offset : overhang - offset + tok_rows]
        d_glu = d_glu + taps_f[offset] * shifted
        tap_rows.append(jnp.sum(gated * shifted, axis=0))
    grad_taps = summed_everywhere(jnp.stack(tap_rows), *SP) * grad_scale
    grad_value = (d_glu * gate_proj).astype(jnp.bfloat16)
    grad_gate = (d_glu * gated * (1.0 - gate_proj)).astype(jnp.bfloat16)
    return (grad_value, grad_gate, grad_out_weight, grad_taps)


def solution(mesh):
    split = Mesh(mesh.devices.reshape(12, 8, mesh.shape["tp"]), ("sp_0", "sp_1", "tp"))
    return jax.shard_map(
        local,
        mesh=split,
        in_specs=(
            P(SP, "tp"),
            P(SP, "tp"),
            P(SP, "tp"),
            P(None, "tp"),
            P("tp"),
            P("tp", None),
            P(SP, None),
        ),
        out_specs=(P(SP, "tp"), P(SP, "tp"), P("tp", SP), P(None, "tp")),
        check_vma=False,
    )
```

```python
import functools
import math

import jax
import jax.numpy as jnp
from jax import lax
from jax.experimental import pallas as pl
from jax.experimental.pallas import tpu as pltpu
from jax.sharding import Mesh
from jax.sharding import PartitionSpec as P

SP = ("sp_0", "sp_1")


norm_eps = 1e-05


def from_everyone(x, axis):
    size = lax.axis_size(axis)
    return lax.all_to_all(jnp.broadcast_to(x[None], (size, *x.shape)), axis, 0, 0, tiled=True)


def taken_together(x, axis):
    return from_everyone(x, axis).sum(axis=0)


def shared_rows(a, b, axis):
    return from_everyone(jnp.concatenate([a, b]).reshape(8, -1), axis)


def summed_everywhere(x, outer, inner):
    size = lax.axis_size(inner)
    rows, width = x.shape
    each = -(-rows // size)
    padded = jnp.pad(x, ((0, each * size - rows), (0, 0))).reshape(size, each, width)
    part = lax.all_to_all(padded, inner, 0, 0, tiled=True).sum(axis=0)
    part = taken_together(part, outer)
    return from_everyone(part, inner).reshape(each * size, width)[:rows]


def passed_along(block, axis, distance):
    devices = range(lax.axis_size(axis))
    route = [(i - distance, i) for i in devices if i - distance in devices]
    return lax.ppermute(block, axis, route)


def column(lanes, rows):
    turned = lanes.T
    return jnp.concatenate([turned[:, r : r + 1] for r in rows], axis=0)


def weight_grad_kernel(model_width, groups, shared_ref, conv_ref, gain_ref, cot_ref, out_ref, act_ref):
    totals = jnp.sum(shared_ref[...], axis=0) / model_width
    mean = column(totals, range(4))
    square = column(totals, range(4, 8))
    inv_std = lax.rsqrt(square - mean * mean + norm_eps)
    centered = (conv_ref[...].astype(jnp.float32) - mean) * inv_std
    normed = centered * gain_ref[...].astype(jnp.float32)
    act_ref[...] = (normed * jax.nn.sigmoid(normed)).astype(jnp.bfloat16)
    inner, each = out_ref.shape[0], out_ref.shape[2]
    block = groups * inner * each

    def one(i, carry):
        rows = pl.ds(pl.multiple_of(i * block, block), block)
        res = jnp.dot(cot_ref[rows, :], act_ref[...], preferred_element_type=jnp.float32)
        for g in range(groups):
            for y in range(inner):
                at = (g * inner + y) * each
                out_ref[y, i * groups + g] = res[at : at + each]
        return carry

    lax.fori_loop(0, cot_ref.shape[0] // block, one, 0)


def weight_grad(shared, conv_saved, gain, cot_t, outer, inner):
    model_width, width = cot_t.shape[0], conv_saved.shape[1]
    each = model_width // (outer * inner)
    return pl.pallas_call(
        functools.partial(weight_grad_kernel, model_width, 2),
        out_shape=jax.ShapeDtypeStruct((inner, outer, each, width), jnp.float32),
        scratch_shapes=[pltpu.VMEM(conv_saved.shape, jnp.bfloat16)],
        cost_estimate=pl.CostEstimate(
            flops=2 * conv_saved.size * model_width,
            bytes_accessed=2 * cot_t.size + 4 * model_width * width,
            transcendentals=conv_saved.size,
        ),
        compiler_params=pltpu.CompilerParams(vmem_limit_bytes=16 * 2**20),
        name="weight_grad",
    )(shared, conv_saved, gain, cot_t)


def local(proj_value, proj_gate, conv_saved, conv_taps, norm_gain, out_weight, cotangent):
    model_width = cotangent.shape[1]
    tok_rows = cotangent.shape[0]
    tap_count = conv_taps.shape[0]
    overhang = tap_count - 1
    grad_scale = 1.0 / math.sqrt(tok_rows * lax.axis_size(SP))
    outer, inner = (lax.axis_size(a) for a in SP)
    d_act = lax.dot_general(
        cotangent, out_weight, (((1,), (1,)), ((), ())), preferred_element_type=jnp.float32
    )
    d_act = lax.optimization_barrier(d_act)
    conv_f = conv_saved.astype(jnp.float32)
    shared = shared_rows(jnp.sum(conv_f, axis=1), jnp.sum(conv_f * conv_f, axis=1), "tp")
    terms = weight_grad(shared, conv_saved, norm_gain[None], cotangent.T, outer, inner)
    term = lax.psum_scatter(terms, SP[1], scatter_dimension=0)
    term = lax.psum_scatter(term, SP[0], scatter_dimension=0)
    grad_out_weight = term.T * grad_scale
    totals = shared.sum(axis=0).reshape(2, tok_rows)
    row_mean = totals[0] / model_width
    row_var = totals[1] / model_width - row_mean * row_mean
    inv_std = lax.rsqrt(row_var + norm_eps)
    centered = (conv_f - row_mean[:, None]) * inv_std[:, None]
    gain_f = norm_gain.astype(jnp.float32)
    normed = centered * gain_f
    gate_norm = jax.nn.sigmoid(normed)
    d_hat = d_act * gate_norm * (1.0 + normed * (1.0 - gate_norm)) * gain_f
    moments = shared_rows(jnp.sum(d_hat, axis=1), jnp.sum(d_hat * centered, axis=1), "tp")
    moments = moments.sum(axis=0).reshape(2, tok_rows)
    first = moments[0] / model_width
    second = moments[1] / model_width
    d_conv = inv_std[:, None] * (d_hat - first[:, None] - centered * second[:, None])
    ahead = passed_along(d_conv[:overhang], SP, -1)
    extended = jnp.concatenate([d_conv, ahead], axis=0)
    gate_proj = jax.nn.sigmoid(proj_gate.astype(jnp.float32))
    gated = proj_value.astype(jnp.float32) * gate_proj
    taps_f = conv_taps.astype(jnp.float32)
    d_glu = jnp.zeros_like(d_conv)
    tap_rows = []
    for offset in range(tap_count):
        shifted = extended[overhang - offset : overhang - offset + tok_rows]
        d_glu = d_glu + taps_f[offset] * shifted
        tap_rows.append(jnp.sum(gated * shifted, axis=0))
    grad_taps = summed_everywhere(jnp.stack(tap_rows), *SP) * grad_scale
    grad_value = (d_glu * gate_proj).astype(jnp.bfloat16)
    grad_gate = (d_glu * gated * (1.0 - gate_proj)).astype(jnp.bfloat16)
    return (grad_value, grad_gate, grad_out_weight, grad_taps)


def solution(mesh):
    split = Mesh(mesh.devices.reshape(12, 8, mesh.shape["tp"]), ("sp_0", "sp_1", "tp"))
    return jax.shard_map(
        local,
        mesh=split,
        in_specs=(
            P(SP, "tp"),
            P(SP, "tp"),
            P(SP, "tp"),
            P(None, "tp"),
            P("tp"),
            P("tp", None),
            P(SP, None),
        ),
        out_specs=(P(SP, "tp"), P(SP, "tp"), P("tp", SP), P(None, "tp")),
        check_vma=False,
    )
```

```python
import functools
import math

import jax
import jax.numpy as jnp
from jax import lax
from jax.experimental import pallas as pl
from jax.experimental.pallas import tpu as pltpu
from jax.sharding import Mesh
from jax.sharding import PartitionSpec as P

SP = ("z_hi", "z_lo", "y_hi", "y_lo")
FAR = ("z_hi", "y_hi")
NEAR = ("z_lo", "y_lo")


norm_eps = 1e-05


def from_everyone(x, axis):
    size = lax.axis_size(axis)
    return lax.all_to_all(jnp.broadcast_to(x[None], (size, *x.shape)), axis, 0, 0, tiled=True)


def taken_together(x, axis):
    return from_everyone(x, axis).sum(axis=0)


def shared_rows(a, b, axis):
    return from_everyone(jnp.concatenate([a, b]).reshape(8, -1), axis)


def scattered_sum(x, axes):
    size = lax.axis_size(axes)
    rows, width = x.shape
    each = -(-rows // size)
    padded = jnp.pad(x, ((0, each * size - rows), (0, 0))).reshape(size, each, width)
    return lax.all_to_all(padded, axes, 0, 0, tiled=True).sum(axis=0)


def from_neighbour(block, apart):
    route = [(2 * z + y, 2 * (z ^ apart[0]) + (y ^ apart[1])) for z in range(2) for y in range(2)]
    return lax.ppermute(block, NEAR, route)


def passed_along(block, axis, distance):
    devices = range(lax.axis_size(axis))
    route = [(i - distance, i) for i in devices if i - distance in devices]
    return lax.ppermute(block, axis, route)


def column(lanes, rows):
    turned = lanes.T
    return jnp.concatenate([turned[:, r : r + 1] for r in rows], axis=0)


APART = ((0, 0), (0, 1), (1, 0), (1, 1))


def weight_grad_kernel(model_width, z_size, shared_ref, conv_ref, gain_ref, cot_ref, *rest):
    *out_refs, act_ref, all_ref = rest
    totals = jnp.sum(shared_ref[...], axis=0) / model_width
    mean = column(totals, range(4))
    square = column(totals, range(4, 8))
    inv_std = lax.rsqrt(square - mean * mean + norm_eps)
    centered = (conv_ref[...].astype(jnp.float32) - mean) * inv_std
    normed = centered * gain_ref[...].astype(jnp.float32)
    act_ref[...] = (normed * jax.nn.sigmoid(normed)).astype(jnp.bfloat16)
    chunks, each = all_ref.shape[:2]
    together = 16
    block = together * each

    def one(i, carry):
        rows = pl.ds(pl.multiple_of(i * block, block), block)
        res = jnp.dot(cot_ref[rows, :], act_ref[...], preferred_element_type=jnp.float32)
        for g in range(together):
            all_ref[i * together + g] = res[g * each : (g + 1) * each]
        return carry

    lax.fori_loop(0, chunks // together, one, 0)
    z_lo, y_lo = (lax.axis_index(a) for a in NEAR)
    y_half = chunks // z_size // 2
    for (dz, dy), out_ref in zip(APART, out_refs):
        z_at = z_lo + dz - 2 * dz * z_lo
        y_at = y_lo + dy - 2 * dy * y_lo
        for z_hi in range(z_size // 2):
            for y_hi in range(y_half):
                at = (z_hi * y_half + y_hi) * each
                out_ref[at : at + each] = all_ref[((2 * z_hi + z_at) * y_half + y_hi) * 2 + y_at]


def weight_grad(shared, conv_saved, gain, cot_t, z_size, y_size):
    model_width, width = cot_t.shape[0], conv_saved.shape[1]
    chunks = z_size * y_size
    each = model_width // chunks
    part = jax.ShapeDtypeStruct((model_width // 4, width), jnp.float32)
    return pl.pallas_call(
        functools.partial(weight_grad_kernel, model_width, z_size),
        out_shape=(part,) * 4,
        scratch_shapes=[
            pltpu.VMEM(conv_saved.shape, jnp.bfloat16),
            pltpu.VMEM((chunks, each, width), jnp.float32),
        ],
        cost_estimate=pl.CostEstimate(
            flops=2 * conv_saved.size * model_width,
            bytes_accessed=2 * cot_t.size + 4 * model_width * width,
            transcendentals=conv_saved.size,
        ),
        compiler_params=pltpu.CompilerParams(vmem_limit_bytes=20 * 2**20),
        name="weight_grad",
    )(shared, conv_saved, gain, cot_t)


def local(proj_value, proj_gate, conv_saved, conv_taps, norm_gain, out_weight, cotangent):
    model_width = cotangent.shape[1]
    tok_rows = cotangent.shape[0]
    tap_count = conv_taps.shape[0]
    overhang = tap_count - 1
    grad_scale = 1.0 / math.sqrt(tok_rows * lax.axis_size(SP))
    z_size, y_size = lax.axis_size(SP[:2]), lax.axis_size(SP[2:])
    d_act = lax.dot_general(
        cotangent, out_weight, (((1,), (1,)), ((), ())), preferred_element_type=jnp.float32
    )
    conv_f = conv_saved.astype(jnp.float32)
    shared = shared_rows(jnp.sum(conv_f, axis=1), jnp.sum(conv_f * conv_f, axis=1), "tp")
    shared, d_act = lax.optimization_barrier((shared, d_act))
    parts = weight_grad(shared, conv_saved, norm_gain[None], cotangent.T, z_size, y_size)
    totals = shared.sum(axis=0).reshape(2, tok_rows)
    row_mean = totals[0] / model_width
    row_var = totals[1] / model_width - row_mean * row_mean
    inv_std = lax.rsqrt(row_var + norm_eps)
    centered = (conv_f - row_mean[:, None]) * inv_std[:, None]
    gain_f = norm_gain.astype(jnp.float32)
    normed = centered * gain_f
    gate_norm = jax.nn.sigmoid(normed)
    d_hat = d_act * gate_norm * (1.0 + normed * (1.0 - gate_norm)) * gain_f
    moments = shared_rows(jnp.sum(d_hat, axis=1), jnp.sum(d_hat * centered, axis=1), "tp")
    moments, parts = lax.optimization_barrier((moments, parts))
    terms = parts[0] + sum(from_neighbour(p, d) for p, d in zip(parts[1:], APART[1:]))
    terms = terms.reshape(z_size * y_size // 4, -1, terms.shape[1])
    moments = moments.sum(axis=0).reshape(2, tok_rows)
    first = moments[0] / model_width
    second = moments[1] / model_width
    d_conv = inv_std[:, None] * (d_hat - first[:, None] - centered * second[:, None])
    ahead = passed_along(d_conv[:overhang], SP, -1)
    extended = jnp.concatenate([d_conv, ahead], axis=0)
    gate_proj = jax.nn.sigmoid(proj_gate.astype(jnp.float32))
    gated = proj_value.astype(jnp.float32) * gate_proj
    taps_f = conv_taps.astype(jnp.float32)
    d_glu = jnp.zeros_like(d_conv)
    tap_rows = []
    for offset in range(tap_count):
        shifted = extended[overhang - offset : overhang - offset + tok_rows]
        d_glu = d_glu + taps_f[offset] * shifted
        tap_rows.append(jnp.sum(gated * shifted, axis=0))
    tap_part = taken_together(scattered_sum(jnp.stack(tap_rows), FAR), NEAR)
    each = terms.shape[1]
    spread = jnp.broadcast_to(tap_part[None], (terms.shape[0], *tap_part.shape))
    arrived = lax.all_to_all(jnp.concatenate([terms, spread], axis=1), FAR, 0, 0, tiled=True)
    grad_out_weight = arrived[:, :each].sum(axis=0).T * grad_scale
    grad_taps = arrived[:, each:].reshape(-1, arrived.shape[2])[:tap_count] * grad_scale
    grad_value = (d_glu * gate_proj).astype(jnp.bfloat16)
    grad_gate = (d_glu * gated * (1.0 - gate_proj)).astype(jnp.bfloat16)
    return (grad_value, grad_gate, grad_out_weight, grad_taps)


def solution(mesh):
    split = Mesh(mesh.devices.reshape(6, 2, 4, 2, mesh.shape["tp"]), (*SP, "tp"))
    return jax.shard_map(
        local,
        mesh=split,
        in_specs=(
            P(SP, "tp"),
            P(SP, "tp"),
            P(SP, "tp"),
            P(None, "tp"),
            P("tp"),
            P("tp", None),
            P(SP, None),
        ),
        out_specs=(P(SP, "tp"), P(SP, "tp"), P("tp", SP), P(None, "tp")),
        check_vma=False,
    )
```

```python
import functools
import math

import jax
import jax.numpy as jnp
from jax import lax
from jax.experimental import pallas as pl
from jax.experimental.pallas import tpu as pltpu
from jax.sharding import Mesh
from jax.sharding import PartitionSpec as P

SP = ("z_hi", "z_lo", "y_hi", "y_lo")
FAR = ("z_hi", "y_hi")
NEAR = ("z_lo", "y_lo")


norm_eps = 1e-05


def from_everyone(x, axis):
    size = lax.axis_size(axis)
    return lax.all_to_all(jnp.broadcast_to(x[None], (size, *x.shape)), axis, 0, 0, tiled=True)


def taken_together(x, axis):
    return from_everyone(x, axis).sum(axis=0)


def shared_rows(a, b, axis):
    return from_everyone(jnp.concatenate([a, b]).reshape(8, -1), axis)


def scattered_sum(x, axes):
    size = lax.axis_size(axes)
    rows, width = x.shape
    each = -(-rows // size)
    padded = jnp.pad(x, ((0, each * size - rows), (0, 0))).reshape(size, each, width)
    return lax.all_to_all(padded, axes, 0, 0, tiled=True).sum(axis=0)


def from_neighbour(block, apart):
    route = [(2 * z + y, 2 * (z ^ apart[0]) + (y ^ apart[1])) for z in range(2) for y in range(2)]
    return lax.ppermute(block, NEAR, route)


def passed_along(block, axis, distance):
    devices = range(lax.axis_size(axis))
    route = [(i - distance, i) for i in devices if i - distance in devices]
    return lax.ppermute(block, axis, route)


def column(lanes, rows):
    turned = lanes.T
    return jnp.concatenate([turned[:, r : r + 1] for r in rows], axis=0)


APART = ((0, 0), (0, 1), (1, 0), (1, 1))


def weight_grad_kernel(model_width, z_size, shared_ref, conv_ref, gain_ref, cot_ref, *rest):
    *out_refs, act_ref, all_ref = rest
    totals = jnp.sum(shared_ref[...], axis=0) / model_width
    mean = column(totals, range(4))
    square = column(totals, range(4, 8))
    inv_std = lax.rsqrt(square - mean * mean + norm_eps)
    centered = (conv_ref[...].astype(jnp.float32) - mean) * inv_std
    normed = centered * gain_ref[...].astype(jnp.float32)
    act_ref[...] = (normed * jax.nn.sigmoid(normed)).astype(jnp.bfloat16)
    chunks, each = all_ref.shape[:2]
    together = 16
    block = together * each

    def one(i, carry):
        rows = pl.ds(pl.multiple_of(i * block, block), block)
        res = jnp.dot(cot_ref[rows, :], act_ref[...], preferred_element_type=jnp.float32)
        for g in range(together):
            all_ref[i * together + g] = res[g * each : (g + 1) * each]
        return carry

    lax.fori_loop(0, chunks // together, one, 0)
    z_lo, y_lo = (lax.axis_index(a) for a in NEAR)
    y_half = chunks // z_size // 2
    for (dz, dy), out_ref in zip(APART, out_refs):
        z_at = z_lo + dz - 2 * dz * z_lo
        y_at = y_lo + dy - 2 * dy * y_lo
        for z_hi in range(z_size // 2):
            for y_hi in range(y_half):
                at = (z_hi * y_half + y_hi) * each
                out_ref[at : at + each] = all_ref[((2 * z_hi + z_at) * y_half + y_hi) * 2 + y_at]


def weight_grad(shared, conv_saved, gain, cot_t, z_size, y_size):
    model_width, width = cot_t.shape[0], conv_saved.shape[1]
    chunks = z_size * y_size
    each = model_width // chunks
    part = jax.ShapeDtypeStruct((model_width // 4, width), jnp.float32)
    return pl.pallas_call(
        functools.partial(weight_grad_kernel, model_width, z_size),
        out_shape=(part,) * 4,
        scratch_shapes=[
            pltpu.VMEM(conv_saved.shape, jnp.bfloat16),
            pltpu.VMEM((chunks, each, width), jnp.float32),
        ],
        cost_estimate=pl.CostEstimate(
            flops=2 * conv_saved.size * model_width,
            bytes_accessed=2 * cot_t.size + 4 * model_width * width,
            transcendentals=conv_saved.size,
        ),
        compiler_params=pltpu.CompilerParams(vmem_limit_bytes=20 * 2**20),
        name="weight_grad",
    )(shared, conv_saved, gain, cot_t)


STEP = 32


def filter_rows(window, value, gate, taps_ref, tap_sums_ref):
    tap_count = taps_ref.shape[0]
    gate_proj = jax.nn.sigmoid(gate.astype(jnp.float32))
    gated = value.astype(jnp.float32) * gate_proj
    d_glu = jnp.zeros_like(gated)
    for phase in range(8):
        turned = window[phase : phase + 2 * STEP - 8]
        for at in range(phase, tap_count, 8):
            k = tap_count - 1 - at
            shifted = turned[at - phase : at - phase + STEP]
            d_glu += taps_ref[k : k + 1].astype(jnp.float32) * shifted
            tap_sums_ref[k] += (gated * shifted).reshape(STEP // 8, 8, -1).sum(axis=0)
    grad_value = d_glu * gate_proj
    grad_gate = d_glu * gated * (1.0 - gate_proj)
    return grad_value.astype(jnp.bfloat16), grad_gate.astype(jnp.bfloat16)


def main_rows_kernel(conv_grad_ref, value_ref, gate_ref, taps_ref, value_out, gate_out, tap_out):
    tap_out[...] = jnp.zeros_like(tap_out)

    def one(i, carry):
        at = pl.multiple_of(i * STEP, STEP)
        rows = pl.ds(at, STEP)
        value_out[rows], gate_out[rows] = filter_rows(
            conv_grad_ref[pl.ds(at, 2 * STEP)], value_ref[rows], gate_ref[rows], taps_ref, tap_out
        )
        return carry

    lax.fori_loop(0, value_ref.shape[0] // STEP - 1, one, 0)
    last = value_ref.shape[0] - STEP
    value_out[last:] = jnp.zeros((STEP, value_out.shape[1]), value_out.dtype)
    gate_out[last:] = jnp.zeros((STEP, gate_out.shape[1]), gate_out.dtype)


def last_rows_kernel(
    conv_grad_ref, ahead_ref, value_ref, gate_ref, taps_ref, value_in, gate_in, tap_in, value_out, gate_out, tap_out, sums_ref
):
    last = value_ref.shape[0] - STEP
    width = conv_grad_ref.shape[1]
    ahead = ahead_ref[...]
    fill = jnp.zeros((STEP - ahead.shape[0], width), jnp.float32)
    window = jnp.concatenate([conv_grad_ref[last:], ahead, fill], axis=0)
    sums_ref[...] = tap_in[...]
    value_out[:last] = value_in[:last]
    gate_out[:last] = gate_in[:last]
    value_out[last:], gate_out[last:] = filter_rows(window, value_ref[last:], gate_ref[last:], taps_ref, sums_ref)
    tap_count = taps_ref.shape[0]
    tap_out[:tap_count] = jnp.sum(sums_ref[...], axis=1)
    tap_out[tap_count:] = jnp.zeros((tap_out.shape[0] - tap_count, width), jnp.float32)


def main_rows(conv_grad, value, gate, taps):
    grad = jax.ShapeDtypeStruct(value.shape, jnp.bfloat16)
    return pl.pallas_call(
        main_rows_kernel,
        out_shape=(grad, grad, jax.ShapeDtypeStruct((taps.shape[0], 8, taps.shape[1]), jnp.float32)),
        cost_estimate=pl.CostEstimate(flops=4 * taps.shape[0] * value.size, bytes_accessed=12 * value.size, transcendentals=value.size),
        compiler_params=pltpu.CompilerParams(vmem_limit_bytes=12 * 2**20),
        name="main_rows",
    )(conv_grad, value, gate, taps)


def last_rows(conv_grad, ahead, value, gate, taps, done, padded_taps):
    grad = jax.ShapeDtypeStruct(value.shape, jnp.bfloat16)
    return pl.pallas_call(
        last_rows_kernel,
        out_shape=(grad, grad, jax.ShapeDtypeStruct((padded_taps, taps.shape[1]), jnp.float32)),
        scratch_shapes=[pltpu.VMEM(done[2].shape, jnp.float32)],
        cost_estimate=pl.CostEstimate(flops=4 * taps.size * STEP, bytes_accessed=16 * value.size, transcendentals=0),
        compiler_params=pltpu.CompilerParams(vmem_limit_bytes=12 * 2**20),
        name="last_rows",
    )(conv_grad, ahead, value, gate, taps, *done)


def local(proj_value, proj_gate, conv_saved, conv_taps, norm_gain, out_weight, cotangent):
    model_width = cotangent.shape[1]
    tok_rows = cotangent.shape[0]
    tap_count = conv_taps.shape[0]
    overhang = tap_count - 1
    grad_scale = 1.0 / math.sqrt(tok_rows * lax.axis_size(SP))
    z_size, y_size = lax.axis_size(SP[:2]), lax.axis_size(SP[2:])
    d_act = lax.dot_general(
        cotangent, out_weight, (((1,), (1,)), ((), ())), preferred_element_type=jnp.float32
    )
    conv_f = conv_saved.astype(jnp.float32)
    shared = shared_rows(jnp.sum(conv_f, axis=1), jnp.sum(conv_f * conv_f, axis=1), "tp")
    shared, d_act = lax.optimization_barrier((shared, d_act))
    parts = weight_grad(shared, conv_saved, norm_gain[None], cotangent.T, z_size, y_size)
    totals = shared.sum(axis=0).reshape(2, tok_rows)
    row_mean = totals[0] / model_width
    row_var = totals[1] / model_width - row_mean * row_mean
    inv_std = lax.rsqrt(row_var + norm_eps)
    centered = (conv_f - row_mean[:, None]) * inv_std[:, None]
    gain_f = norm_gain.astype(jnp.float32)
    normed = centered * gain_f
    gate_norm = jax.nn.sigmoid(normed)
    d_hat = d_act * gate_norm * (1.0 + normed * (1.0 - gate_norm)) * gain_f
    moments = shared_rows(jnp.sum(d_hat, axis=1), jnp.sum(d_hat * centered, axis=1), "tp")
    moments, _ = lax.optimization_barrier((moments, parts[0]))
    terms = parts[0] + sum(from_neighbour(p, d) for p, d in zip(parts[1:], APART[1:]))
    terms = terms.reshape(z_size * y_size // 4, -1, terms.shape[1])
    moments = moments.sum(axis=0).reshape(2, tok_rows)
    first = moments[0] / model_width
    second = moments[1] / model_width
    d_conv = inv_std[:, None] * (d_hat - first[:, None] - centered * second[:, None])
    ahead = passed_along(d_conv[:overhang], SP, -1)
    done = main_rows(d_conv, proj_value, proj_gate, conv_taps)
    far = lax.axis_size(FAR)
    padded_taps = -(-tap_count // far) * far
    grad_value, grad_gate, tap_sums = last_rows(d_conv, ahead, proj_value, proj_gate, conv_taps, done, padded_taps)
    tap_part = taken_together(scattered_sum(tap_sums, FAR), NEAR)
    each = terms.shape[1]
    spread = jnp.broadcast_to(tap_part[None], (terms.shape[0], *tap_part.shape))
    arrived = lax.all_to_all(jnp.concatenate([terms, spread], axis=1), FAR, 0, 0, tiled=True)
    grad_out_weight = arrived[:, :each].sum(axis=0).T * grad_scale
    grad_taps = arrived[:, each:].reshape(-1, arrived.shape[2])[:tap_count] * grad_scale
    return (grad_value, grad_gate, grad_out_weight, grad_taps)


def solution(mesh):
    split = Mesh(mesh.devices.reshape(6, 2, 4, 2, mesh.shape["tp"]), (*SP, "tp"))
    return jax.shard_map(
        local,
        mesh=split,
        in_specs=(
            P(SP, "tp"),
            P(SP, "tp"),
            P(SP, "tp"),
            P(None, "tp"),
            P("tp"),
            P("tp", None),
            P(SP, None),
        ),
        out_specs=(P(SP, "tp"), P(SP, "tp"), P("tp", SP), P(None, "tp")),
        check_vma=False,
    )
```

```python
import functools
import math

import jax
import jax.numpy as jnp
from jax import lax
from jax.experimental import pallas as pl
from jax.experimental.pallas import tpu as pltpu
from jax.sharding import Mesh
from jax.sharding import PartitionSpec as P

SP = ("z", "y")

norm_eps = 1e-05


def from_everyone(x, axis):
    size = lax.axis_size(axis)
    return lax.all_to_all(jnp.broadcast_to(x[None], (size, *x.shape)), axis, 0, 0, tiled=True)


def taken_together(x, axis):
    return from_everyone(x, axis).sum(axis=0)


def shared_rows(a, b, axis):
    return from_everyone(jnp.concatenate([a, b]).reshape(8, -1), axis)


def scattered_sum(x, axes):
    size = lax.axis_size(axes)
    rows, width = x.shape
    each = -(-rows // size)
    padded = jnp.pad(x, ((0, each * size - rows), (0, 0))).reshape(size, each, width)
    return lax.all_to_all(padded, axes, 0, 0, tiled=True).sum(axis=0)


def passed_along(block, axis, distance):
    devices = range(lax.axis_size(axis))
    route = [(i - distance, i) for i in devices if i - distance in devices]
    return lax.ppermute(block, axis, route)


def column(lanes, rows):
    turned = lanes.T
    return jnp.concatenate([turned[:, r : r + 1] for r in rows], axis=0)


def weight_grad_kernel(model_width, groups, shared_ref, conv_ref, gain_ref, cot_ref, out_ref, act_ref):
    totals = jnp.sum(shared_ref[...], axis=0) / model_width
    mean = column(totals, range(4))
    square = column(totals, range(4, 8))
    inv_std = lax.rsqrt(square - mean * mean + norm_eps)
    centered = (conv_ref[...].astype(jnp.float32) - mean) * inv_std
    normed = centered * gain_ref[...].astype(jnp.float32)
    act_ref[...] = (normed * jax.nn.sigmoid(normed)).astype(jnp.bfloat16)
    inner, each = out_ref.shape[0], out_ref.shape[2]
    block = groups * inner * each

    def one(i, carry):
        rows = pl.ds(pl.multiple_of(i * block, block), block)
        res = jnp.dot(cot_ref[rows, :], act_ref[...], preferred_element_type=jnp.float32)
        for g in range(groups):
            for y in range(inner):
                at = (g * inner + y) * each
                out_ref[y, i * groups + g] = res[at : at + each]
        return carry

    lax.fori_loop(0, cot_ref.shape[0] // block, one, 0)


def weight_grad(shared, conv_saved, gain, cot_t, outer, inner):
    model_width, width = cot_t.shape[0], conv_saved.shape[1]
    each = model_width // (outer * inner)
    return pl.pallas_call(
        functools.partial(weight_grad_kernel, model_width, 2),
        out_shape=jax.ShapeDtypeStruct((inner, outer, each, width), jnp.float32),
        scratch_shapes=[pltpu.VMEM(conv_saved.shape, jnp.bfloat16)],
        cost_estimate=pl.CostEstimate(
            flops=2 * conv_saved.size * model_width,
            bytes_accessed=2 * cot_t.size + 4 * model_width * width,
            transcendentals=conv_saved.size,
        ),
        compiler_params=pltpu.CompilerParams(vmem_limit_bytes=16 * 2**20),
        name="weight_grad",
    )(shared, conv_saved, gain, cot_t)


STEP = 32


def filter_rows(window, value, gate, taps_ref, tap_sums_ref):
    tap_count = taps_ref.shape[0]
    gate_proj = jax.nn.sigmoid(gate.astype(jnp.float32))
    gated = value.astype(jnp.float32) * gate_proj
    d_glu = jnp.zeros_like(gated)
    for phase in range(8):
        turned = window[phase : phase + 2 * STEP - 8]
        for at in range(phase, tap_count, 8):
            k = tap_count - 1 - at
            shifted = turned[at - phase : at - phase + STEP]
            d_glu += taps_ref[k : k + 1].astype(jnp.float32) * shifted
            tap_sums_ref[k] += (gated * shifted).reshape(STEP // 8, 8, -1).sum(axis=0)
    grad_value = d_glu * gate_proj
    grad_gate = d_glu * gated * (1.0 - gate_proj)
    return grad_value.astype(jnp.bfloat16), grad_gate.astype(jnp.bfloat16)


def main_rows_kernel(conv_grad_ref, value_ref, gate_ref, taps_ref, value_out, gate_out, tap_out):
    tap_out[...] = jnp.zeros_like(tap_out)

    def one(i, carry):
        at = pl.multiple_of(i * STEP, STEP)
        rows = pl.ds(at, STEP)
        value_out[rows], gate_out[rows] = filter_rows(
            conv_grad_ref[pl.ds(at, 2 * STEP)], value_ref[rows], gate_ref[rows], taps_ref, tap_out
        )
        return carry

    lax.fori_loop(0, value_ref.shape[0] // STEP - 1, one, 0)
    last = value_ref.shape[0] - STEP
    value_out[last:] = jnp.zeros((STEP, value_out.shape[1]), value_out.dtype)
    gate_out[last:] = jnp.zeros((STEP, gate_out.shape[1]), gate_out.dtype)


def last_rows_kernel(
    conv_grad_ref, ahead_ref, value_ref, gate_ref, taps_ref, value_in, gate_in, tap_in, value_out, gate_out, tap_out, sums_ref
):
    last = value_ref.shape[0] - STEP
    width = conv_grad_ref.shape[1]
    ahead = ahead_ref[...]
    fill = jnp.zeros((STEP - ahead.shape[0], width), jnp.float32)
    window = jnp.concatenate([conv_grad_ref[last:], ahead, fill], axis=0)
    sums_ref[...] = tap_in[...]
    value_out[:last] = value_in[:last]
    gate_out[:last] = gate_in[:last]
    value_out[last:], gate_out[last:] = filter_rows(window, value_ref[last:], gate_ref[last:], taps_ref, sums_ref)
    tap_count = taps_ref.shape[0]
    tap_out[:tap_count] = jnp.sum(sums_ref[...], axis=1)
    tap_out[tap_count:] = jnp.zeros((tap_out.shape[0] - tap_count, width), jnp.float32)


def main_rows(conv_grad, value, gate, taps):
    grad = jax.ShapeDtypeStruct(value.shape, jnp.bfloat16)
    return pl.pallas_call(
        main_rows_kernel,
        out_shape=(grad, grad, jax.ShapeDtypeStruct((taps.shape[0], 8, taps.shape[1]), jnp.float32)),
        cost_estimate=pl.CostEstimate(flops=4 * taps.shape[0] * value.size, bytes_accessed=12 * value.size, transcendentals=value.size),
        compiler_params=pltpu.CompilerParams(vmem_limit_bytes=12 * 2**20),
        name="main_rows",
    )(conv_grad, value, gate, taps)


def last_rows(conv_grad, ahead, value, gate, taps, done, padded_taps):
    grad = jax.ShapeDtypeStruct(value.shape, jnp.bfloat16)
    return pl.pallas_call(
        last_rows_kernel,
        out_shape=(grad, grad, jax.ShapeDtypeStruct((padded_taps, taps.shape[1]), jnp.float32)),
        scratch_shapes=[pltpu.VMEM(done[2].shape, jnp.float32)],
        cost_estimate=pl.CostEstimate(flops=4 * taps.size * STEP, bytes_accessed=16 * value.size, transcendentals=0),
        compiler_params=pltpu.CompilerParams(vmem_limit_bytes=12 * 2**20),
        name="last_rows",
    )(conv_grad, ahead, value, gate, taps, *done)


def local(proj_value, proj_gate, conv_saved, conv_taps, norm_gain, out_weight, cotangent):
    model_width = cotangent.shape[1]
    tok_rows = cotangent.shape[0]
    tap_count = conv_taps.shape[0]
    overhang = tap_count - 1
    grad_scale = 1.0 / math.sqrt(tok_rows * lax.axis_size(SP))
    z_size, y_size = (lax.axis_size(a) for a in SP)
    d_act = lax.dot_general(
        cotangent, out_weight, (((1,), (1,)), ((), ())), preferred_element_type=jnp.float32
    )
    conv_f = conv_saved.astype(jnp.float32)
    shared = shared_rows(jnp.sum(conv_f, axis=1), jnp.sum(conv_f * conv_f, axis=1), "tp")
    shared, d_act = lax.optimization_barrier((shared, d_act))
    terms = weight_grad(shared, conv_saved, norm_gain[None], cotangent.T, z_size, y_size)
    terms = lax.psum_scatter(terms, "y", scatter_dimension=0)
    totals = shared.sum(axis=0).reshape(2, tok_rows)
    row_mean = totals[0] / model_width
    row_var = totals[1] / model_width - row_mean * row_mean
    inv_std = lax.rsqrt(row_var + norm_eps)
    centered = (conv_f - row_mean[:, None]) * inv_std[:, None]
    gain_f = norm_gain.astype(jnp.float32)
    normed = centered * gain_f
    gate_norm = jax.nn.sigmoid(normed)
    d_hat = d_act * gate_norm * (1.0 + normed * (1.0 - gate_norm)) * gain_f
    moments = shared_rows(jnp.sum(d_hat, axis=1), jnp.sum(d_hat * centered, axis=1), "tp")
    moments = moments.sum(axis=0).reshape(2, tok_rows)
    first = moments[0] / model_width
    second = moments[1] / model_width
    d_conv = inv_std[:, None] * (d_hat - first[:, None] - centered * second[:, None])
    ahead = passed_along(d_conv[:overhang], SP, -1)
    done = main_rows(d_conv, proj_value, proj_gate, conv_taps)
    padded_taps = -(-tap_count // z_size) * z_size
    grad_value, grad_gate, tap_sums = last_rows(d_conv, ahead, proj_value, proj_gate, conv_taps, done, padded_taps)
    tap_part = taken_together(scattered_sum(tap_sums, "z"), "y")
    each = terms.shape[1]
    spread = jnp.broadcast_to(tap_part[None], (z_size, *tap_part.shape))
    arrived = lax.all_to_all(jnp.concatenate([terms, spread], axis=1), "z", 0, 0, tiled=True)
    grad_out_weight = arrived[:, :each].sum(axis=0).T * grad_scale
    grad_taps = arrived[:, each:].reshape(-1, arrived.shape[2])[:tap_count] * grad_scale
    return (grad_value, grad_gate, grad_out_weight, grad_taps)


def solution(mesh):
    split = Mesh(mesh.devices.reshape(12, 8, mesh.shape["tp"]), (*SP, "tp"))
    return jax.shard_map(
        local,
        mesh=split,
        in_specs=(
            P(SP, "tp"),
            P(SP, "tp"),
            P(SP, "tp"),
            P(None, "tp"),
            P("tp"),
            P("tp", None),
            P(SP, None),
        ),
        out_specs=(P(SP, "tp"), P(SP, "tp"), P("tp", SP), P(None, "tp")),
        check_vma=False,
    )
```

```python
import functools
import math

import jax
import jax.numpy as jnp
from jax import lax
from jax.experimental import pallas as pl
from jax.experimental.pallas import tpu as pltpu
from jax.sharding import Mesh
from jax.sharding import PartitionSpec as P

SP = ("z", "y")

norm_eps = 1e-05


def from_everyone(x, axis):
    size = lax.axis_size(axis)
    return lax.all_to_all(jnp.broadcast_to(x[None], (size, *x.shape)), axis, 0, 0, tiled=True)


def taken_together(x, axis):
    return from_everyone(x, axis).sum(axis=0)


def scattered_sum(x, axes):
    size = lax.axis_size(axes)
    rows, width = x.shape
    each = -(-rows // size)
    padded = jnp.pad(x, ((0, each * size - rows), (0, 0))).reshape(size, each, width)
    return lax.all_to_all(padded, axes, 0, 0, tiled=True).sum(axis=0)


def passed_along(block, axis, distance):
    devices = range(lax.axis_size(axis))
    route = [(i - distance, i) for i in devices if i - distance in devices]
    return lax.ppermute(block, axis, route)


def column(lanes, rows):
    turned = lanes.T
    return jnp.concatenate([turned[:, r : r + 1] for r in rows], axis=0)


def spread_rows(first, second, out_ref):
    columns = [c[at : at + 128] for c in (first, second) for at in range(0, c.shape[0], 128)]
    rows = jnp.concatenate(columns, axis=1).T
    for i in range(out_ref.shape[0]):
        out_ref[i] = rows


def statistics_kernel(conv_ref, out_ref):
    conv = conv_ref[...].astype(jnp.float32)
    spread_rows(jnp.sum(conv, axis=1, keepdims=True), jnp.sum(conv * conv, axis=1, keepdims=True), out_ref)


def statistics(conv_saved, devices):
    return pl.pallas_call(
        statistics_kernel,
        out_shape=jax.ShapeDtypeStruct((devices, conv_saved.shape[0] // 64, 128), jnp.float32),
        cost_estimate=pl.CostEstimate(flops=3 * conv_saved.size, bytes_accessed=2 * conv_saved.size, transcendentals=0),
        compiler_params=pltpu.CompilerParams(vmem_limit_bytes=8 * 2**20),
        name="statistics",
    )(conv_saved)


def standardized(model_width, shared_ref, conv_ref):
    totals = jnp.sum(shared_ref[...], axis=0) / model_width
    half = totals.shape[0] // 2
    mean = column(totals, range(half))
    square = column(totals, range(half, 2 * half))
    inv_std = lax.rsqrt(square - mean * mean + norm_eps)
    return (conv_ref[...].astype(jnp.float32) - mean) * inv_std


def norm_grad_kernel(model_width, shared_ref, conv_ref, gain_ref, act_grad_ref, hat_ref, out_ref):
    centered = standardized(model_width, shared_ref, conv_ref)
    gain = gain_ref[...].astype(jnp.float32)
    normed = centered * gain
    gate_norm = jax.nn.sigmoid(normed)
    d_hat = act_grad_ref[...] * gate_norm * (1.0 + normed * (1.0 - gate_norm)) * gain
    hat_ref[...] = d_hat
    spread_rows(jnp.sum(d_hat, axis=1, keepdims=True), jnp.sum(d_hat * centered, axis=1, keepdims=True), out_ref)


def norm_grad(model_width, shared, conv_saved, gain, act_grad):
    return pl.pallas_call(
        functools.partial(norm_grad_kernel, model_width),
        out_shape=(jax.ShapeDtypeStruct(conv_saved.shape, jnp.float32), jax.ShapeDtypeStruct(shared.shape, jnp.float32)),
        cost_estimate=pl.CostEstimate(
            flops=20 * conv_saved.size, bytes_accessed=10 * conv_saved.size, transcendentals=conv_saved.size
        ),
        compiler_params=pltpu.CompilerParams(vmem_limit_bytes=8 * 2**20),
        name="norm_grad",
    )(shared, conv_saved, gain, act_grad)


def weight_grad_kernel(model_width, z_size, shared_ref, conv_ref, gain_ref, cot_ref, out_ref, act_ref):
    centered = standardized(model_width, shared_ref, conv_ref)
    normed = centered * gain_ref[...].astype(jnp.float32)
    act_ref[...] = (normed * jax.nn.sigmoid(normed)).astype(jnp.bfloat16)
    y_size = out_ref.shape[0]
    each = out_ref.shape[1] // z_size
    block = 2 * y_size * each
    for i in range(z_size // 2):
        res = jnp.dot(cot_ref[i * block : (i + 1) * block], act_ref[...], preferred_element_type=jnp.float32)
        for g in range(2):
            for y in range(y_size):
                at, to = (g * y_size + y) * each, (2 * i + g) * each
                out_ref[y, to : to + each] = res[at : at + each]


def weight_grad(shared, conv_saved, gain, cot_t, z_size, y_size):
    model_width, width = cot_t.shape[0], conv_saved.shape[1]
    return pl.pallas_call(
        functools.partial(weight_grad_kernel, model_width, z_size),
        out_shape=jax.ShapeDtypeStruct((y_size, model_width // y_size, width), jnp.float32),
        scratch_shapes=[pltpu.VMEM(conv_saved.shape, jnp.bfloat16)],
        cost_estimate=pl.CostEstimate(
            flops=2 * conv_saved.size * model_width,
            bytes_accessed=2 * cot_t.size + 4 * model_width * width,
            transcendentals=conv_saved.size,
        ),
        compiler_params=pltpu.CompilerParams(vmem_limit_bytes=16 * 2**20),
        name="weight_grad",
    )(shared, conv_saved, gain, cot_t)


STEP = 32


def widen(taps_ref, wide_ref):
    for k in range(taps_ref.shape[0]):
        wide_ref[k] = jnp.broadcast_to(taps_ref[k : k + 1].astype(jnp.float32), wide_ref.shape[1:])


def filter_rows(window, value, gate, wide_ref, tap_sums_ref):
    tap_count = wide_ref.shape[0]
    gate_proj = jax.nn.sigmoid(gate.astype(jnp.float32))
    gated = value.astype(jnp.float32) * gate_proj
    groups = (STEP // 8, 8, gated.shape[1])
    gated_groups = gated.reshape(groups)
    d_glu = jnp.zeros(groups, jnp.float32)
    for phase in range(8):
        turned = window[phase : phase + 2 * STEP - 8]
        for at in range(phase, tap_count, 8):
            k = tap_count - 1 - at
            shifted = turned[at - phase : at - phase + STEP].reshape(groups)
            d_glu += wide_ref[k] * shifted
            tap_sums_ref[k] += (gated_groups * shifted).sum(axis=0)
    d_glu = d_glu.reshape(gated.shape)
    grad_value = d_glu * gate_proj
    grad_gate = d_glu * gated * (1.0 - gate_proj)
    return grad_value.astype(jnp.bfloat16), grad_gate.astype(jnp.bfloat16)


def main_rows_kernel(conv_grad_ref, value_ref, gate_ref, taps_ref, value_out, gate_out, tap_out, wide_ref):
    tap_out[...] = jnp.zeros_like(tap_out)
    widen(taps_ref, wide_ref)

    def one(i, carry):
        at = pl.multiple_of(i * STEP, STEP)
        rows = pl.ds(at, STEP)
        value_out[rows], gate_out[rows] = filter_rows(
            conv_grad_ref[pl.ds(at, 2 * STEP)], value_ref[rows], gate_ref[rows], wide_ref, tap_out
        )
        return carry

    lax.fori_loop(0, value_ref.shape[0] // STEP - 1, one, 0)
    last = value_ref.shape[0] - STEP
    value_out[last:] = jnp.zeros((STEP, value_out.shape[1]), value_out.dtype)
    gate_out[last:] = jnp.zeros((STEP, gate_out.shape[1]), gate_out.dtype)


def last_rows_kernel(
    conv_grad_ref, ahead_ref, value_ref, gate_ref, taps_ref, value_in, gate_in, tap_in, value_out, gate_out, tap_out, sums_ref, wide_ref
):
    last = value_ref.shape[0] - STEP
    width = conv_grad_ref.shape[1]
    ahead = ahead_ref[...]
    fill = jnp.zeros((STEP - ahead.shape[0], width), jnp.float32)
    window = jnp.concatenate([conv_grad_ref[last:], ahead, fill], axis=0)
    sums_ref[...] = tap_in[...]
    widen(taps_ref, wide_ref)
    value_out[:last] = value_in[:last]
    gate_out[:last] = gate_in[:last]
    value_out[last:], gate_out[last:] = filter_rows(window, value_ref[last:], gate_ref[last:], wide_ref, sums_ref)
    tap_count = taps_ref.shape[0]
    tap_out[:tap_count] = jnp.sum(sums_ref[...], axis=1)
    tap_out[tap_count:] = jnp.zeros((tap_out.shape[0] - tap_count, width), jnp.float32)


def main_rows(conv_grad, value, gate, taps):
    grad = jax.ShapeDtypeStruct(value.shape, jnp.bfloat16)
    return pl.pallas_call(
        main_rows_kernel,
        out_shape=(grad, grad, jax.ShapeDtypeStruct((taps.shape[0], 8, taps.shape[1]), jnp.float32)),
        scratch_shapes=[pltpu.VMEM((taps.shape[0], 8, taps.shape[1]), jnp.float32)],
        cost_estimate=pl.CostEstimate(flops=4 * taps.shape[0] * value.size, bytes_accessed=12 * value.size, transcendentals=value.size),
        compiler_params=pltpu.CompilerParams(vmem_limit_bytes=12 * 2**20),
        name="main_rows",
    )(conv_grad, value, gate, taps)


def last_rows(conv_grad, ahead, value, gate, taps, done, padded_taps):
    grad = jax.ShapeDtypeStruct(value.shape, jnp.bfloat16)
    return pl.pallas_call(
        last_rows_kernel,
        out_shape=(grad, grad, jax.ShapeDtypeStruct((padded_taps, taps.shape[1]), jnp.float32)),
        scratch_shapes=[pltpu.VMEM(done[2].shape, jnp.float32)] * 2,
        cost_estimate=pl.CostEstimate(flops=4 * taps.size * STEP, bytes_accessed=16 * value.size, transcendentals=0),
        compiler_params=pltpu.CompilerParams(vmem_limit_bytes=12 * 2**20),
        name="last_rows",
    )(conv_grad, ahead, value, gate, taps, *done)


def local(proj_value, proj_gate, conv_saved, conv_taps, norm_gain, out_weight, cotangent):
    model_width = cotangent.shape[1]
    tok_rows = cotangent.shape[0]
    tap_count = conv_taps.shape[0]
    overhang = tap_count - 1
    grad_scale = 1.0 / math.sqrt(tok_rows * lax.axis_size(SP))
    z_size, y_size = (lax.axis_size(a) for a in SP)
    d_act = lax.dot_general(
        cotangent, out_weight, (((1,), (1,)), ((), ())), preferred_element_type=jnp.float32
    )
    everyone = lambda x: lax.all_to_all(x, "tp", 0, 0, tiled=True)
    shared = everyone(statistics(conv_saved, lax.axis_size("tp")))
    shared, d_act = lax.optimization_barrier((shared, d_act))
    terms = weight_grad(shared, conv_saved, norm_gain[None], cotangent.T, z_size, y_size)
    terms = lax.psum_scatter(terms, "y", scatter_dimension=0)
    terms = terms.reshape(z_size, -1, terms.shape[1])
    d_hat, moments = norm_grad(model_width, shared, conv_saved, norm_gain[None], d_act)
    moments = everyone(moments)
    totals = shared.sum(axis=0).reshape(2, tok_rows)
    row_mean = totals[0] / model_width
    row_var = totals[1] / model_width - row_mean * row_mean
    inv_std = lax.rsqrt(row_var + norm_eps)
    centered = (conv_saved.astype(jnp.float32) - row_mean[:, None]) * inv_std[:, None]
    moments = moments.sum(axis=0).reshape(2, tok_rows)
    first = moments[0] / model_width
    second = moments[1] / model_width
    d_conv = inv_std[:, None] * (d_hat - first[:, None] - centered * second[:, None])
    ahead = passed_along(d_conv[:overhang], SP, -1)
    done = main_rows(d_conv, proj_value, proj_gate, conv_taps)
    padded_taps = -(-tap_count // z_size) * z_size
    grad_value, grad_gate, tap_sums = last_rows(d_conv, ahead, proj_value, proj_gate, conv_taps, done, padded_taps)
    tap_part = taken_together(scattered_sum(tap_sums, "z"), "y")
    each = terms.shape[1]
    spread = jnp.broadcast_to(tap_part[None], (z_size, *tap_part.shape))
    arrived = lax.all_to_all(jnp.concatenate([terms, spread], axis=1), "z", 0, 0, tiled=True)
    grad_out_weight = arrived[:, :each].sum(axis=0).T * grad_scale
    grad_taps = arrived[:, each:].reshape(-1, arrived.shape[2])[:tap_count] * grad_scale
    return (grad_value, grad_gate, grad_out_weight, grad_taps)


def solution(mesh):
    split = Mesh(mesh.devices.reshape(12, 8, mesh.shape["tp"]), (*SP, "tp"))
    return jax.shard_map(
        local,
        mesh=split,
        in_specs=(
            P(SP, "tp"),
            P(SP, "tp"),
            P(SP, "tp"),
            P(None, "tp"),
            P("tp"),
            P("tp", None),
            P(SP, None),
        ),
        out_specs=(P(SP, "tp"), P(SP, "tp"), P("tp", SP), P(None, "tp")),
        check_vma=False,
    )
```

```python
import functools
import math

import jax
import jax.numpy as jnp
from jax import lax
from jax.experimental import pallas as pl
from jax.experimental.pallas import tpu as pltpu
from jax.sharding import Mesh
from jax.sharding import PartitionSpec as P

SP = ("z", "y")

norm_eps = 1e-05


def from_everyone(x, axis):
    size = lax.axis_size(axis)
    return lax.all_to_all(jnp.broadcast_to(x[None], (size, *x.shape)), axis, 0, 0, tiled=True)


def taken_together(x, axis):
    return from_everyone(x, axis).sum(axis=0)


def scattered_sum(x, axes):
    size = lax.axis_size(axes)
    rows, width = x.shape
    each = -(-rows // size)
    padded = jnp.pad(x, ((0, each * size - rows), (0, 0))).reshape(size, each, width)
    return lax.all_to_all(padded, axes, 0, 0, tiled=True).sum(axis=0)


def passed_along(block, axis, distance):
    devices = range(lax.axis_size(axis))
    route = [(i - distance, i) for i in devices if i - distance in devices]
    return lax.ppermute(block, axis, route)


def column(lanes, rows):
    turned = lanes.T
    return jnp.concatenate([turned[:, r : r + 1] for r in rows], axis=0)


def spread_rows(first, second, out_ref):
    columns = [c[at : at + 128] for c in (first, second) for at in range(0, c.shape[0], 128)]
    rows = jnp.concatenate(columns, axis=1).T
    for i in range(out_ref.shape[0]):
        out_ref[i] = rows


def statistics_kernel(conv_ref, out_ref, held_ref, sems):
    parts = sems.shape[0]
    rows = held_ref.shape[0] // parts
    copies = []
    for i in range(parts):
        part = pl.ds(i * rows, rows)
        copies.append(pltpu.make_async_copy(conv_ref.at[part], held_ref.at[part], sems.at[i]))
        copies[i].start()
    sums, squares = [], []
    for i in range(parts):
        copies[i].wait()
        conv = held_ref[i * rows : (i + 1) * rows].astype(jnp.float32)
        sums.append(jnp.sum(conv, axis=1, keepdims=True))
        squares.append(jnp.sum(conv * conv, axis=1, keepdims=True))
    spread_rows(jnp.concatenate(sums, axis=0), jnp.concatenate(squares, axis=0), out_ref)


def statistics(conv_saved, devices):
    return pl.pallas_call(
        statistics_kernel,
        out_shape=jax.ShapeDtypeStruct((devices, conv_saved.shape[0] // 64, 128), jnp.float32),
        cost_estimate=pl.CostEstimate(flops=3 * conv_saved.size, bytes_accessed=2 * conv_saved.size, transcendentals=0),
        in_specs=[pl.BlockSpec(memory_space=pltpu.HBM)],
        scratch_shapes=[pltpu.VMEM(conv_saved.shape, conv_saved.dtype), pltpu.SemaphoreType.DMA((4,))],
        compiler_params=pltpu.CompilerParams(vmem_limit_bytes=58 * 2**20),
        name="statistics",
    )(conv_saved)


def standardized(model_width, shared_ref, conv_ref):
    totals = jnp.sum(shared_ref[...], axis=0) / model_width
    half = totals.shape[0] // 2
    mean = column(totals, range(half))
    square = column(totals, range(half, 2 * half))
    inv_std = lax.rsqrt(square - mean * mean + norm_eps)
    return (conv_ref[...].astype(jnp.float32) - mean) * inv_std


def norm_grad_kernel(model_width, shared_ref, conv_ref, gain_ref, act_grad_ref, hat_ref, out_ref):
    centered = standardized(model_width, shared_ref, conv_ref)
    gain = gain_ref[...].astype(jnp.float32)
    normed = centered * gain
    gate_norm = jax.nn.sigmoid(normed)
    d_hat = act_grad_ref[...] * gate_norm * (1.0 + normed * (1.0 - gate_norm)) * gain
    hat_ref[...] = d_hat
    spread_rows(jnp.sum(d_hat, axis=1, keepdims=True), jnp.sum(d_hat * centered, axis=1, keepdims=True), out_ref)


def norm_grad(model_width, shared, conv_saved, gain, act_grad):
    return pl.pallas_call(
        functools.partial(norm_grad_kernel, model_width),
        out_shape=(jax.ShapeDtypeStruct(conv_saved.shape, jnp.float32), jax.ShapeDtypeStruct(shared.shape, jnp.float32)),
        cost_estimate=pl.CostEstimate(
            flops=20 * conv_saved.size, bytes_accessed=10 * conv_saved.size, transcendentals=conv_saved.size
        ),
        compiler_params=pltpu.CompilerParams(vmem_limit_bytes=8 * 2**20),
        name="norm_grad",
    )(shared, conv_saved, gain, act_grad)


def weight_grad_kernel(model_width, z_size, shared_ref, conv_ref, gain_ref, cot_ref, out_ref, act_ref, held_ref, sems):
    centered = standardized(model_width, shared_ref, conv_ref)
    normed = centered * gain_ref[...].astype(jnp.float32)
    act_ref[...] = (normed * jax.nn.sigmoid(normed)).astype(jnp.bfloat16)
    y_size = out_ref.shape[0]
    each = out_ref.shape[1] // z_size
    block = 2 * y_size * each
    early = z_size * 2 // 3 * each
    copies = [
        pltpu.make_async_copy(held_ref.at[:, part], out_ref.at[:, part], sems.at[j])
        for j, part in enumerate((pl.ds(0, early), pl.ds(early, z_size * each - early)))
    ]
    for i in range(z_size // 2):
        if 2 * i * each == early:
            copies[0].start()
        res = jnp.dot(cot_ref[i * block : (i + 1) * block], act_ref[...], preferred_element_type=jnp.float32)
        for g in range(2):
            for y in range(y_size):
                at, to = (g * y_size + y) * each, (2 * i + g) * each
                held_ref[y, to : to + each] = res[at : at + each]
    copies[1].start()
    copies[0].wait()
    copies[1].wait()


def weight_grad(shared, conv_saved, gain, cot_t, z_size, y_size):
    model_width, width = cot_t.shape[0], conv_saved.shape[1]
    return pl.pallas_call(
        functools.partial(weight_grad_kernel, model_width, z_size),
        out_shape=jax.ShapeDtypeStruct((y_size, model_width // y_size, width), jnp.float32),
        out_specs=pl.BlockSpec(memory_space=pltpu.HBM),
        scratch_shapes=[
            pltpu.VMEM(conv_saved.shape, jnp.bfloat16),
            pltpu.VMEM((y_size, model_width // y_size, width), jnp.float32),
            pltpu.SemaphoreType.DMA((2,)),
        ],
        cost_estimate=pl.CostEstimate(
            flops=2 * conv_saved.size * model_width,
            bytes_accessed=2 * cot_t.size + 4 * model_width * width,
            transcendentals=conv_saved.size,
        ),
        compiler_params=pltpu.CompilerParams(vmem_limit_bytes=10 * 2**20),
        name="weight_grad",
    )(shared, conv_saved, gain, cot_t)


STEP = 32


def widen(taps_ref, wide_ref):
    for k in range(taps_ref.shape[0]):
        wide_ref[k] = jnp.broadcast_to(taps_ref[k : k + 1].astype(jnp.float32), wide_ref.shape[1:])


def filter_rows(window, value, gate, wide_ref, tap_sums_ref):
    tap_count = wide_ref.shape[0]
    gate_proj = jax.nn.sigmoid(gate.astype(jnp.float32))
    gated = value.astype(jnp.float32) * gate_proj
    groups = (STEP // 8, 8, gated.shape[1])
    gated_groups = gated.reshape(groups)
    d_glu = jnp.zeros(groups, jnp.float32)
    for phase in range(8):
        turned = window[phase : phase + 2 * STEP - 8]
        for at in range(phase, tap_count, 8):
            k = tap_count - 1 - at
            shifted = turned[at - phase : at - phase + STEP].reshape(groups)
            d_glu += wide_ref[k] * shifted
            tap_sums_ref[k] += (gated_groups * shifted).sum(axis=0)
    d_glu = d_glu.reshape(gated.shape)
    grad_value = d_glu * gate_proj
    grad_gate = d_glu * gated * (1.0 - gate_proj)
    return grad_value.astype(jnp.bfloat16), grad_gate.astype(jnp.bfloat16)


def main_rows_kernel(conv_grad_ref, value_ref, gate_ref, taps_ref, value_out, gate_out, tap_out, wide_ref):
    tap_out[...] = jnp.zeros_like(tap_out)
    widen(taps_ref, wide_ref)

    def one(i, carry):
        at = pl.multiple_of(i * STEP, STEP)
        rows = pl.ds(at, STEP)
        value_out[rows], gate_out[rows] = filter_rows(
            conv_grad_ref[pl.ds(at, 2 * STEP)], value_ref[rows], gate_ref[rows], wide_ref, tap_out
        )
        return carry

    lax.fori_loop(0, value_ref.shape[0] // STEP - 1, one, 0)
    last = value_ref.shape[0] - STEP
    value_out[last:] = jnp.zeros((STEP, value_out.shape[1]), value_out.dtype)
    gate_out[last:] = jnp.zeros((STEP, gate_out.shape[1]), gate_out.dtype)


def last_rows_kernel(
    conv_grad_ref, ahead_ref, value_ref, gate_ref, taps_ref, value_in, gate_in, tap_in, value_out, gate_out, tap_out, sums_ref, wide_ref
):
    last = value_ref.shape[0] - STEP
    width = conv_grad_ref.shape[1]
    ahead = ahead_ref[...]
    fill = jnp.zeros((STEP - ahead.shape[0], width), jnp.float32)
    window = jnp.concatenate([conv_grad_ref[last:], ahead, fill], axis=0)
    sums_ref[...] = tap_in[...]
    widen(taps_ref, wide_ref)
    value_out[:last] = value_in[:last]
    gate_out[:last] = gate_in[:last]
    value_out[last:], gate_out[last:] = filter_rows(window, value_ref[last:], gate_ref[last:], wide_ref, sums_ref)
    tap_count = taps_ref.shape[0]
    tap_out[:tap_count] = jnp.sum(sums_ref[...], axis=1)
    tap_out[tap_count:] = jnp.zeros((tap_out.shape[0] - tap_count, width), jnp.float32)


def main_rows(conv_grad, value, gate, taps):
    grad = jax.ShapeDtypeStruct(value.shape, jnp.bfloat16)
    return pl.pallas_call(
        main_rows_kernel,
        out_shape=(grad, grad, jax.ShapeDtypeStruct((taps.shape[0], 8, taps.shape[1]), jnp.float32)),
        scratch_shapes=[pltpu.VMEM((taps.shape[0], 8, taps.shape[1]), jnp.float32)],
        cost_estimate=pl.CostEstimate(flops=4 * taps.shape[0] * value.size, bytes_accessed=12 * value.size, transcendentals=value.size),
        compiler_params=pltpu.CompilerParams(vmem_limit_bytes=12 * 2**20),
        name="main_rows",
    )(conv_grad, value, gate, taps)


def last_rows(conv_grad, ahead, value, gate, taps, done, padded_taps):
    grad = jax.ShapeDtypeStruct(value.shape, jnp.bfloat16)
    return pl.pallas_call(
        last_rows_kernel,
        out_shape=(grad, grad, jax.ShapeDtypeStruct((padded_taps, taps.shape[1]), jnp.float32)),
        scratch_shapes=[pltpu.VMEM(done[2].shape, jnp.float32)] * 2,
        cost_estimate=pl.CostEstimate(flops=4 * taps.size * STEP, bytes_accessed=16 * value.size, transcendentals=0),
        compiler_params=pltpu.CompilerParams(vmem_limit_bytes=12 * 2**20),
        name="last_rows",
    )(conv_grad, ahead, value, gate, taps, *done)


def closing_kernel(scale, arrived_ref, weight_out, tap_out):
    each = weight_out.shape[0]
    total = arrived_ref[0]
    for z in range(1, arrived_ref.shape[0]):
        total = total + arrived_ref[z]
    weight_out[...] = total[:each] * scale
    rows = arrived_ref.shape[1] - each
    for z in range(arrived_ref.shape[0]):
        at = z * rows
        count = min(rows, tap_out.shape[0] - at)
        if count > 0:
            tap_out[at : at + count] = arrived_ref[z, each : each + count] * scale


def closing(arrived, scale, each, tap_count):
    width = arrived.shape[2]
    return pl.pallas_call(
        functools.partial(closing_kernel, scale),
        out_shape=(jax.ShapeDtypeStruct((each, width), jnp.float32), jax.ShapeDtypeStruct((tap_count, width), jnp.float32)),
        cost_estimate=pl.CostEstimate(flops=arrived.size, bytes_accessed=4 * arrived.size, transcendentals=0),
        compiler_params=pltpu.CompilerParams(vmem_limit_bytes=4 * 2**20),
        name="closing",
    )(arrived)


def local(proj_value, proj_gate, conv_saved, conv_taps, norm_gain, out_weight, cotangent):
    model_width = cotangent.shape[1]
    tok_rows = cotangent.shape[0]
    tap_count = conv_taps.shape[0]
    overhang = tap_count - 1
    grad_scale = 1.0 / math.sqrt(tok_rows * lax.axis_size(SP))
    z_size, y_size = (lax.axis_size(a) for a in SP)
    d_act = lax.dot_general(
        cotangent, out_weight, (((1,), (1,)), ((), ())), preferred_element_type=jnp.float32
    )
    everyone = lambda x: lax.all_to_all(x, "tp", 0, 0, tiled=True)
    shared = everyone(statistics(conv_saved, lax.axis_size("tp")))
    shared, d_act = lax.optimization_barrier((shared, d_act))
    terms = weight_grad(shared, conv_saved, norm_gain[None], cotangent.T, z_size, y_size)
    terms = lax.psum_scatter(terms, "y", scatter_dimension=0)
    terms = terms.reshape(z_size, -1, terms.shape[1])
    d_hat, moments = norm_grad(model_width, shared, conv_saved, norm_gain[None], d_act)
    moments = everyone(moments)
    totals = shared.sum(axis=0).reshape(2, tok_rows)
    row_mean = totals[0] / model_width
    row_var = totals[1] / model_width - row_mean * row_mean
    inv_std = lax.rsqrt(row_var + norm_eps)
    centered = (conv_saved.astype(jnp.float32) - row_mean[:, None]) * inv_std[:, None]
    moments = moments.sum(axis=0).reshape(2, tok_rows)
    first = moments[0] / model_width
    second = moments[1] / model_width
    d_conv = inv_std[:, None] * (d_hat - first[:, None] - centered * second[:, None])
    ahead = passed_along(d_conv[:overhang], SP, -1)
    done = main_rows(d_conv, proj_value, proj_gate, conv_taps)
    padded_taps = -(-tap_count // z_size) * z_size
    grad_value, grad_gate, tap_sums = last_rows(d_conv, ahead, proj_value, proj_gate, conv_taps, done, padded_taps)
    tap_part = taken_together(scattered_sum(tap_sums, "z"), "y")
    each = terms.shape[1]
    spread = jnp.broadcast_to(tap_part[None], (z_size, *tap_part.shape))
    arrived = lax.all_to_all(jnp.concatenate([terms, spread], axis=1), "z", 0, 0, tiled=True)
    weight_rows, grad_taps = closing(arrived, grad_scale, each, tap_count)
    grad_out_weight = weight_rows.T
    return (grad_value, grad_gate, grad_out_weight, grad_taps)


def solution(mesh):
    split = Mesh(mesh.devices.reshape(12, 8, mesh.shape["tp"]), (*SP, "tp"))
    return jax.shard_map(
        local,
        mesh=split,
        in_specs=(
            P(SP, "tp"),
            P(SP, "tp"),
            P(SP, "tp"),
            P(None, "tp"),
            P("tp"),
            P("tp", None),
            P(SP, None),
        ),
        out_specs=(P(SP, "tp"), P(SP, "tp"), P("tp", SP), P(None, "tp")),
        check_vma=False,
    )
```

```python
import functools
import math

import jax
import jax.numpy as jnp
from jax import lax
from jax.experimental import pallas as pl
from jax.experimental.pallas import tpu as pltpu
from jax.sharding import Mesh
from jax.sharding import PartitionSpec as P

SP = ("z", "y")

norm_eps = 1e-05


def from_everyone(x, axis):
    size = lax.axis_size(axis)
    return lax.all_to_all(jnp.broadcast_to(x[None], (size, *x.shape)), axis, 0, 0, tiled=True)


def taken_together(x, axis):
    return from_everyone(x, axis).sum(axis=0)


def scattered_sum(x, axes):
    size = lax.axis_size(axes)
    rows, width = x.shape
    each = -(-rows // size)
    padded = jnp.pad(x, ((0, each * size - rows), (0, 0))).reshape(size, each, width)
    return lax.all_to_all(padded, axes, 0, 0, tiled=True).sum(axis=0)


def passed_along(block, axis, distance):
    devices = range(lax.axis_size(axis))
    route = [(i - distance, i) for i in devices if i - distance in devices]
    return lax.ppermute(block, axis, route)


def column(lanes, rows):
    turned = lanes.T
    return jnp.concatenate([turned[:, r : r + 1] for r in rows], axis=0)


def spread_rows(first, second, out_ref):
    columns = [c[at : at + 128] for c in (first, second) for at in range(0, c.shape[0], 128)]
    rows = jnp.concatenate(columns, axis=1).T
    for i in range(out_ref.shape[0]):
        out_ref[i] = rows


def statistics_kernel(conv_ref, out_ref):
    conv = conv_ref[...].astype(jnp.float32)
    spread_rows(jnp.sum(conv, axis=1, keepdims=True), jnp.sum(conv * conv, axis=1, keepdims=True), out_ref)


def statistics(conv_saved, devices):
    return pl.pallas_call(
        statistics_kernel,
        out_shape=jax.ShapeDtypeStruct((devices, conv_saved.shape[0] // 64, 128), jnp.float32),
        cost_estimate=pl.CostEstimate(flops=3 * conv_saved.size, bytes_accessed=2 * conv_saved.size, transcendentals=0),
        compiler_params=pltpu.CompilerParams(vmem_limit_bytes=8 * 2**20),
        name="statistics",
    )(conv_saved)


def standardized(model_width, shared_ref, conv_ref):
    totals = jnp.sum(shared_ref[...], axis=0) / model_width
    half = totals.shape[0] // 2
    mean = column(totals, range(half))
    square = column(totals, range(half, 2 * half))
    inv_std = lax.rsqrt(square - mean * mean + norm_eps)
    return (conv_ref[...].astype(jnp.float32) - mean) * inv_std


def norm_grad_kernel(model_width, shared_ref, conv_ref, gain_ref, act_grad_ref, hat_ref, out_ref):
    centered = standardized(model_width, shared_ref, conv_ref)
    gain = gain_ref[...].astype(jnp.float32)
    normed = centered * gain
    gate_norm = jax.nn.sigmoid(normed)
    d_hat = act_grad_ref[...] * gate_norm * (1.0 + normed * (1.0 - gate_norm)) * gain
    hat_ref[...] = d_hat
    spread_rows(jnp.sum(d_hat, axis=1, keepdims=True), jnp.sum(d_hat * centered, axis=1, keepdims=True), out_ref)


def norm_grad(model_width, shared, conv_saved, gain, act_grad):
    return pl.pallas_call(
        functools.partial(norm_grad_kernel, model_width),
        out_shape=(jax.ShapeDtypeStruct(conv_saved.shape, jnp.float32), jax.ShapeDtypeStruct(shared.shape, jnp.float32)),
        cost_estimate=pl.CostEstimate(
            flops=20 * conv_saved.size, bytes_accessed=10 * conv_saved.size, transcendentals=conv_saved.size
        ),
        compiler_params=pltpu.CompilerParams(vmem_limit_bytes=8 * 2**20),
        name="norm_grad",
    )(shared, conv_saved, gain, act_grad)


def weight_grad_kernel(model_width, z_size, shared_ref, conv_ref, gain_ref, cot_ref, out_ref, act_ref):
    centered = standardized(model_width, shared_ref, conv_ref)
    normed = centered * gain_ref[...].astype(jnp.float32)
    act_ref[...] = (normed * jax.nn.sigmoid(normed)).astype(jnp.bfloat16)
    y_size = out_ref.shape[0]
    each = out_ref.shape[1] // z_size
    block = 2 * y_size * each
    for i in range(z_size // 2):
        res = jnp.dot(cot_ref[i * block : (i + 1) * block], act_ref[...], preferred_element_type=jnp.float32)
        for g in range(2):
            for y in range(y_size):
                at, to = (g * y_size + y) * each, (2 * i + g) * each
                out_ref[y, to : to + each] = res[at : at + each]


def weight_grad(shared, conv_saved, gain, cot_t, z_size, y_size):
    model_width, width = cot_t.shape[0], conv_saved.shape[1]
    return pl.pallas_call(
        functools.partial(weight_grad_kernel, model_width, z_size),
        out_shape=jax.ShapeDtypeStruct((y_size, model_width // y_size, width), jnp.float32),
        scratch_shapes=[pltpu.VMEM(conv_saved.shape, jnp.bfloat16)],
        cost_estimate=pl.CostEstimate(
            flops=2 * conv_saved.size * model_width,
            bytes_accessed=2 * cot_t.size + 4 * model_width * width,
            transcendentals=conv_saved.size,
        ),
        compiler_params=pltpu.CompilerParams(vmem_limit_bytes=16 * 2**20),
        name="weight_grad",
    )(shared, conv_saved, gain, cot_t)


STEP = 32


def widen(taps_ref, wide_ref):
    for k in range(taps_ref.shape[0]):
        wide_ref[k] = jnp.broadcast_to(taps_ref[k : k + 1].astype(jnp.float32), wide_ref.shape[1:])


def shifts(window, first, last):
    for phase in range(8):
        starts = [at for at in range(first, last + 1) if at % 8 == phase]
        turned = window[phase : starts[-1] + STEP]
        for at in starts:
            yield at, turned[at - phase : at - phase + STEP].reshape(STEP // 8, 8, -1)


def gate_of(value, gate):
    gate_proj = jax.nn.sigmoid(gate.astype(jnp.float32))
    return gate_proj, value.astype(jnp.float32) * gate_proj


def tap_sums_kernel(tap_count, conv_grad_ref, behind_ref, value_ref, gate_ref, out_ref, gated_ref, sums_ref):
    sums_ref[...] = jnp.zeros_like(sums_ref)
    gated_ref[:STEP] = behind_ref[...]
    skipped = STEP - (tap_count - 1)

    def one(i, carry):
        at = pl.multiple_of(i * STEP, STEP)
        rows = pl.ds(at, STEP)
        gated_ref[pl.ds(pl.multiple_of(at + STEP, STEP), STEP)] = gate_of(value_ref[rows], gate_ref[rows])[1]
        conv_grad = conv_grad_ref[rows].reshape(STEP // 8, 8, -1)
        window = gated_ref[pl.ds(at, 2 * STEP)]
        for start, shifted in shifts(window, skipped, skipped + tap_count - 1):
            sums_ref[start - skipped] += (conv_grad * shifted).sum(axis=0)
        return carry

    lax.fori_loop(0, value_ref.shape[0] // STEP, one, 0)
    out_ref[:tap_count] = jnp.sum(sums_ref[...], axis=1)
    out_ref[tap_count:] = jnp.zeros((out_ref.shape[0] - tap_count, out_ref.shape[1]), jnp.float32)


def tap_sums(conv_grad, behind, value, gate, tap_count, padded_taps):
    rows, width = value.shape
    return pl.pallas_call(
        functools.partial(tap_sums_kernel, tap_count),
        out_shape=jax.ShapeDtypeStruct((padded_taps, width), jnp.float32),
        scratch_shapes=[
            pltpu.VMEM((rows + STEP, width), jnp.float32),
            pltpu.VMEM((tap_count, 8, width), jnp.float32),
        ],
        cost_estimate=pl.CostEstimate(flops=2 * tap_count * value.size, bytes_accessed=8 * value.size, transcendentals=value.size),
        compiler_params=pltpu.CompilerParams(vmem_limit_bytes=8 * 2**20),
        name="tap_sums",
    )(conv_grad, behind, value, gate)


def filter_kernel(conv_grad_ref, ahead_ref, value_ref, gate_ref, taps_ref, value_out, gate_out, wide_ref):
    tap_count, width = taps_ref.shape
    for k in range(tap_count):
        wide_ref[k] = jnp.broadcast_to(taps_ref[k : k + 1].astype(jnp.float32), wide_ref.shape[1:])

    def filter_rows(window, rows):
        gate_proj, gated = gate_of(value_ref[rows], gate_ref[rows])
        d_glu = jnp.zeros((STEP // 8, 8, width), jnp.float32)
        for start, shifted in shifts(window, 0, tap_count - 1):
            d_glu += wide_ref[tap_count - 1 - start] * shifted
        d_glu = d_glu.reshape(STEP, width)
        value_out[rows] = (d_glu * gate_proj).astype(jnp.bfloat16)
        gate_out[rows] = (d_glu * gated * (1.0 - gate_proj)).astype(jnp.bfloat16)

    def one(i, carry):
        at = pl.multiple_of(i * STEP, STEP)
        filter_rows(conv_grad_ref[pl.ds(at, 2 * STEP)], pl.ds(at, STEP))
        return carry

    last = value_ref.shape[0] - STEP
    lax.fori_loop(0, last // STEP, one, 0)
    ahead = ahead_ref[...]
    fill = jnp.zeros((STEP - ahead.shape[0], width), jnp.float32)
    filter_rows(jnp.concatenate([conv_grad_ref[last:], ahead, fill], axis=0), pl.ds(last, STEP))


def filtered(conv_grad, ahead, value, gate, taps):
    grad = jax.ShapeDtypeStruct(value.shape, jnp.bfloat16)
    return pl.pallas_call(
        filter_kernel,
        out_shape=(grad, grad),
        scratch_shapes=[pltpu.VMEM((taps.shape[0], 8, taps.shape[1]), jnp.float32)],
        cost_estimate=pl.CostEstimate(flops=2 * taps.shape[0] * value.size, bytes_accessed=12 * value.size, transcendentals=value.size),
        compiler_params=pltpu.CompilerParams(vmem_limit_bytes=8 * 2**20),
        name="filtered",
    )(conv_grad, ahead, value, gate, taps)


def closing_kernel(scale, arrived_ref, weight_out, tap_out):
    each = weight_out.shape[0]
    total = arrived_ref[0]
    for z in range(1, arrived_ref.shape[0]):
        total = total + arrived_ref[z]
    weight_out[...] = total[:each] * scale
    rows = arrived_ref.shape[1] - each
    for z in range(arrived_ref.shape[0]):
        at = z * rows
        count = min(rows, tap_out.shape[0] - at)
        if count > 0:
            tap_out[at : at + count] = arrived_ref[z, each : each + count] * scale


def closing(arrived, scale, each, tap_count):
    width = arrived.shape[2]
    return pl.pallas_call(
        functools.partial(closing_kernel, scale),
        out_shape=(jax.ShapeDtypeStruct((each, width), jnp.float32), jax.ShapeDtypeStruct((tap_count, width), jnp.float32)),
        cost_estimate=pl.CostEstimate(flops=arrived.size, bytes_accessed=4 * arrived.size, transcendentals=0),
        compiler_params=pltpu.CompilerParams(vmem_limit_bytes=4 * 2**20),
        name="closing",
    )(arrived)


def local(proj_value, proj_gate, conv_saved, conv_taps, norm_gain, out_weight, cotangent):
    model_width = cotangent.shape[1]
    tok_rows = cotangent.shape[0]
    tap_count = conv_taps.shape[0]
    overhang = tap_count - 1
    grad_scale = 1.0 / math.sqrt(tok_rows * lax.axis_size(SP))
    z_size, y_size = (lax.axis_size(a) for a in SP)
    d_act = lax.dot_general(
        cotangent, out_weight, (((1,), (1,)), ((), ())), preferred_element_type=jnp.float32
    )
    everyone = lambda x: lax.all_to_all(x, "tp", 0, 0, tiled=True)
    shared = everyone(statistics(conv_saved, lax.axis_size("tp")))
    shared, d_act = lax.optimization_barrier((shared, d_act))
    terms = weight_grad(shared, conv_saved, norm_gain[None], cotangent.T, z_size, y_size)
    terms = lax.psum_scatter(terms, "y", scatter_dimension=0)
    terms = terms.reshape(z_size, -1, terms.shape[1])
    d_hat, moments = norm_grad(model_width, shared, conv_saved, norm_gain[None], d_act)
    moments, value_end, gate_end = lax.optimization_barrier((moments, proj_value[-STEP:], proj_gate[-STEP:]))
    moments = everyone(moments)
    behind = passed_along(gate_of(value_end, gate_end)[1], SP, 1)
    totals = shared.sum(axis=0).reshape(2, tok_rows)
    row_mean = totals[0] / model_width
    row_var = totals[1] / model_width - row_mean * row_mean
    inv_std = lax.rsqrt(row_var + norm_eps)
    centered = (conv_saved.astype(jnp.float32) - row_mean[:, None]) * inv_std[:, None]
    moments = moments.sum(axis=0).reshape(2, tok_rows)
    first = moments[0] / model_width
    second = moments[1] / model_width
    d_conv = inv_std[:, None] * (d_hat - first[:, None] - centered * second[:, None])
    padded_taps = -(-tap_count // z_size) * z_size
    sums = tap_sums(d_conv, behind, proj_value, proj_gate, tap_count, padded_taps)
    head, sums = lax.optimization_barrier((d_conv[:overhang], sums))
    ahead = passed_along(head, SP, -1)
    grad_value, grad_gate = filtered(d_conv, ahead, proj_value, proj_gate, conv_taps)
    tap_part = taken_together(scattered_sum(sums, "z"), "y")
    each = terms.shape[1]
    spread = jnp.broadcast_to(tap_part[None], (z_size, *tap_part.shape))
    arrived = lax.all_to_all(jnp.concatenate([terms, spread], axis=1), "z", 0, 0, tiled=True)
    weight_rows, grad_taps = closing(arrived, grad_scale, each, tap_count)
    grad_out_weight = weight_rows.T
    return (grad_value, grad_gate, grad_out_weight, grad_taps)


def solution(mesh):
    split = Mesh(mesh.devices.reshape(12, 8, mesh.shape["tp"]), (*SP, "tp"))
    return jax.shard_map(
        local,
        mesh=split,
        in_specs=(
            P(SP, "tp"),
            P(SP, "tp"),
            P(SP, "tp"),
            P(None, "tp"),
            P("tp"),
            P("tp", None),
            P(SP, None),
        ),
        out_specs=(P(SP, "tp"), P(SP, "tp"), P("tp", SP), P(None, "tp")),
        check_vma=False,
    )
```

```python
import functools
import math

import jax
import jax.numpy as jnp
from jax import lax
from jax.experimental import pallas as pl
from jax.experimental.pallas import tpu as pltpu
from jax.sharding import Mesh
from jax.sharding import PartitionSpec as P

SP = ("z", "y")

norm_eps = 1e-05


def from_everyone(x, axis):
    size = lax.axis_size(axis)
    return lax.all_to_all(jnp.broadcast_to(x[None], (size, *x.shape)), axis, 0, 0, tiled=True)


def taken_together(x, axis):
    return from_everyone(x, axis).sum(axis=0)


def scattered_sum(x, axes):
    size = lax.axis_size(axes)
    rows, width = x.shape
    each = -(-rows // size)
    padded = jnp.pad(x, ((0, each * size - rows), (0, 0))).reshape(size, each, width)
    return lax.all_to_all(padded, axes, 0, 0, tiled=True).sum(axis=0)


def passed_along(block, axis, distance):
    devices = range(lax.axis_size(axis))
    route = [(i - distance, i) for i in devices if i - distance in devices]
    return lax.ppermute(block, axis, route)


def column(lanes, rows):
    turned = lanes.T
    return jnp.concatenate([turned[:, r : r + 1] for r in rows], axis=0)


def spread_rows(first, second, out_ref):
    columns = [c[at : at + 128] for c in (first, second) for at in range(0, c.shape[0], 128)]
    rows = jnp.concatenate(columns, axis=1).T
    for i in range(out_ref.shape[0]):
        out_ref[i] = rows


def statistics_kernel(conv_ref, out_ref):
    conv = conv_ref[...].astype(jnp.float32)
    spread_rows(jnp.sum(conv, axis=1, keepdims=True), jnp.sum(conv * conv, axis=1, keepdims=True), out_ref)


def statistics(conv_saved, devices):
    return pl.pallas_call(
        statistics_kernel,
        out_shape=jax.ShapeDtypeStruct((devices, conv_saved.shape[0] // 64, 128), jnp.float32),
        cost_estimate=pl.CostEstimate(flops=3 * conv_saved.size, bytes_accessed=2 * conv_saved.size, transcendentals=0),
        compiler_params=pltpu.CompilerParams(vmem_limit_bytes=8 * 2**20),
        name="statistics",
    )(conv_saved)


def standardized(model_width, shared_ref, conv_ref):
    totals = jnp.sum(shared_ref[...], axis=0) / model_width
    half = totals.shape[0] // 2
    mean = column(totals, range(half))
    square = column(totals, range(half, 2 * half))
    inv_std = lax.rsqrt(square - mean * mean + norm_eps)
    return (conv_ref[...].astype(jnp.float32) - mean) * inv_std


def norm_grad_kernel(model_width, shared_ref, conv_ref, gain_ref, act_grad_ref, hat_ref, out_ref):
    centered = standardized(model_width, shared_ref, conv_ref)
    gain = gain_ref[...].astype(jnp.float32)
    normed = centered * gain
    gate_norm = jax.nn.sigmoid(normed)
    d_hat = act_grad_ref[...] * gate_norm * (1.0 + normed * (1.0 - gate_norm)) * gain
    hat_ref[...] = d_hat
    spread_rows(jnp.sum(d_hat, axis=1, keepdims=True), jnp.sum(d_hat * centered, axis=1, keepdims=True), out_ref)


def norm_grad(model_width, shared, conv_saved, gain, act_grad):
    return pl.pallas_call(
        functools.partial(norm_grad_kernel, model_width),
        out_shape=(jax.ShapeDtypeStruct(conv_saved.shape, jnp.float32), jax.ShapeDtypeStruct(shared.shape, jnp.float32)),
        cost_estimate=pl.CostEstimate(
            flops=20 * conv_saved.size, bytes_accessed=10 * conv_saved.size, transcendentals=conv_saved.size
        ),
        compiler_params=pltpu.CompilerParams(vmem_limit_bytes=8 * 2**20),
        name="norm_grad",
    )(shared, conv_saved, gain, act_grad)


def weight_grad_kernel(model_width, z_size, shared_ref, conv_ref, gain_ref, cot_ref, out_ref, act_ref):
    centered = standardized(model_width, shared_ref, conv_ref)
    normed = centered * gain_ref[...].astype(jnp.float32)
    act_ref[...] = (normed * jax.nn.sigmoid(normed)).astype(jnp.bfloat16)
    y_size = out_ref.shape[0]
    each = out_ref.shape[1] // z_size
    block = 2 * y_size * each
    for i in range(z_size // 2):
        res = jnp.dot(cot_ref[i * block : (i + 1) * block], act_ref[...], preferred_element_type=jnp.float32)
        for g in range(2):
            for y in range(y_size):
                at, to = (g * y_size + y) * each, (2 * i + g) * each
                out_ref[y, to : to + each] = res[at : at + each]


def weight_grad(shared, conv_saved, gain, cot_t, z_size, y_size):
    model_width, width = cot_t.shape[0], conv_saved.shape[1]
    return pl.pallas_call(
        functools.partial(weight_grad_kernel, model_width, z_size),
        out_shape=jax.ShapeDtypeStruct((y_size, model_width // y_size, width), jnp.float32),
        scratch_shapes=[pltpu.VMEM(conv_saved.shape, jnp.bfloat16)],
        cost_estimate=pl.CostEstimate(
            flops=2 * conv_saved.size * model_width,
            bytes_accessed=2 * cot_t.size + 4 * model_width * width,
            transcendentals=conv_saved.size,
        ),
        compiler_params=pltpu.CompilerParams(vmem_limit_bytes=16 * 2**20),
        name="weight_grad",
    )(shared, conv_saved, gain, cot_t)


STEP = 32


def widen(taps_ref, wide_ref):
    for k in range(taps_ref.shape[0]):
        wide_ref[k] = jnp.broadcast_to(taps_ref[k : k + 1].astype(jnp.float32), wide_ref.shape[1:])


def shifts(window, first, last):
    for phase in range(8):
        starts = [at for at in range(first, last + 1) if at % 8 == phase]
        turned = window[phase : starts[-1] + STEP]
        for at in starts:
            yield at, turned[at - phase : at - phase + STEP].reshape(STEP // 8, 8, -1)


def gate_of(value, gate):
    gate_proj = jax.nn.sigmoid(gate.astype(jnp.float32))
    return gate_proj, value.astype(jnp.float32) * gate_proj


def tap_sums_kernel(tap_count, conv_grad_ref, behind_ref, value_ref, gate_ref, out_ref, gated_ref, sums_ref):
    sums_ref[...] = jnp.zeros_like(sums_ref)
    gated_ref[:STEP] = behind_ref[...]
    skipped = STEP - (tap_count - 1)

    def one(i, carry):
        at = pl.multiple_of(i * STEP, STEP)
        rows = pl.ds(at, STEP)
        gated_ref[pl.ds(pl.multiple_of(at + STEP, STEP), STEP)] = gate_of(value_ref[rows], gate_ref[rows])[1]
        conv_grad = conv_grad_ref[rows].reshape(STEP // 8, 8, -1)
        window = gated_ref[pl.ds(at, 2 * STEP)]
        for start, shifted in shifts(window, skipped, skipped + tap_count - 1):
            sums_ref[start - skipped] += (conv_grad * shifted).sum(axis=0)
        return carry

    lax.fori_loop(0, value_ref.shape[0] // STEP, one, 0)
    out_ref[:tap_count] = jnp.sum(sums_ref[...], axis=1)
    out_ref[tap_count:] = jnp.zeros((out_ref.shape[0] - tap_count, out_ref.shape[1]), jnp.float32)


def tap_sums(conv_grad, behind, value, gate, tap_count, padded_taps):
    rows, width = value.shape
    return pl.pallas_call(
        functools.partial(tap_sums_kernel, tap_count),
        out_shape=jax.ShapeDtypeStruct((padded_taps, width), jnp.float32),
        scratch_shapes=[
            pltpu.VMEM((rows + STEP, width), jnp.float32),
            pltpu.VMEM((tap_count, 8, width), jnp.float32),
        ],
        cost_estimate=pl.CostEstimate(flops=2 * tap_count * value.size, bytes_accessed=8 * value.size, transcendentals=value.size),
        compiler_params=pltpu.CompilerParams(vmem_limit_bytes=8 * 2**20),
        name="tap_sums",
    )(conv_grad, behind, value, gate)


def filter_kernel(conv_grad_ref, ahead_ref, value_ref, gate_ref, taps_ref, value_out, gate_out, wide_ref):
    tap_count, width = taps_ref.shape
    for k in range(tap_count):
        wide_ref[k] = jnp.broadcast_to(taps_ref[k : k + 1].astype(jnp.float32), wide_ref.shape[1:])

    def filter_rows(window, rows):
        gate_proj, gated = gate_of(value_ref[rows], gate_ref[rows])
        d_glu = jnp.zeros((STEP // 8, 8, width), jnp.float32)
        for start, shifted in shifts(window, 0, tap_count - 1):
            d_glu += wide_ref[tap_count - 1 - start] * shifted
        d_glu = d_glu.reshape(STEP, width)
        value_out[rows] = (d_glu * gate_proj).astype(jnp.bfloat16)
        gate_out[rows] = (d_glu * gated * (1.0 - gate_proj)).astype(jnp.bfloat16)

    def one(i, carry):
        at = pl.multiple_of(i * STEP, STEP)
        filter_rows(conv_grad_ref[pl.ds(at, 2 * STEP)], pl.ds(at, STEP))
        return carry

    last = value_ref.shape[0] - STEP
    lax.fori_loop(0, last // STEP, one, 0)
    ahead = ahead_ref[...]
    fill = jnp.zeros((STEP - ahead.shape[0], width), jnp.float32)
    filter_rows(jnp.concatenate([conv_grad_ref[last:], ahead, fill], axis=0), pl.ds(last, STEP))


def filtered(conv_grad, ahead, value, gate, taps):
    grad = jax.ShapeDtypeStruct(value.shape, jnp.bfloat16)
    return pl.pallas_call(
        filter_kernel,
        out_shape=(grad, grad),
        scratch_shapes=[pltpu.VMEM((taps.shape[0], 8, taps.shape[1]), jnp.float32)],
        cost_estimate=pl.CostEstimate(flops=2 * taps.shape[0] * value.size, bytes_accessed=12 * value.size, transcendentals=value.size),
        compiler_params=pltpu.CompilerParams(vmem_limit_bytes=8 * 2**20),
        name="filtered",
    )(conv_grad, ahead, value, gate, taps)


def closing_kernel(scale, arrived_ref, weight_out, tap_out):
    each = weight_out.shape[0]
    total = arrived_ref[0]
    for z in range(1, arrived_ref.shape[0]):
        total = total + arrived_ref[z]
    weight_out[...] = total[:each] * scale
    rows = arrived_ref.shape[1] - each
    for z in range(arrived_ref.shape[0]):
        at = z * rows
        count = min(rows, tap_out.shape[0] - at)
        if count > 0:
            tap_out[at : at + count] = arrived_ref[z, each : each + count] * scale


def closing(arrived, scale, each, tap_count):
    width = arrived.shape[2]
    return pl.pallas_call(
        functools.partial(closing_kernel, scale),
        out_shape=(jax.ShapeDtypeStruct((each, width), jnp.float32), jax.ShapeDtypeStruct((tap_count, width), jnp.float32)),
        cost_estimate=pl.CostEstimate(flops=arrived.size, bytes_accessed=4 * arrived.size, transcendentals=0),
        compiler_params=pltpu.CompilerParams(vmem_limit_bytes=4 * 2**20),
        name="closing",
    )(arrived)


def local(proj_value, proj_gate, conv_saved, conv_taps, norm_gain, out_weight, cotangent):
    model_width = cotangent.shape[1]
    tok_rows = cotangent.shape[0]
    tap_count = conv_taps.shape[0]
    overhang = tap_count - 1
    grad_scale = 1.0 / math.sqrt(tok_rows * lax.axis_size(SP))
    z_size, y_size = (lax.axis_size(a) for a in SP)
    d_act = lax.dot_general(
        cotangent, out_weight, (((1,), (1,)), ((), ())), preferred_element_type=jnp.float32
    )
    everyone = lambda x: lax.all_to_all(x, "tp", 0, 0, tiled=True)
    shared = everyone(statistics(conv_saved, lax.axis_size("tp")))
    shared, d_act = lax.optimization_barrier((shared, d_act))
    terms = weight_grad(shared, conv_saved, norm_gain[None], cotangent.T, z_size, y_size)
    terms = lax.psum_scatter(terms, "y", scatter_dimension=0)
    terms = terms.reshape(z_size, -1, terms.shape[1])
    d_hat, moments = norm_grad(model_width, shared, conv_saved, norm_gain[None], d_act)
    moments, value_end, gate_end = lax.optimization_barrier((moments, proj_value[-STEP:], proj_gate[-STEP:]))
    moments = everyone(moments)
    behind = passed_along(gate_of(value_end, gate_end)[1], SP, 1)
    totals = shared.sum(axis=0).reshape(2, tok_rows)
    row_mean = totals[0] / model_width
    row_var = totals[1] / model_width - row_mean * row_mean
    inv_std = lax.rsqrt(row_var + norm_eps)
    centered = (conv_saved.astype(jnp.float32) - row_mean[:, None]) * inv_std[:, None]
    moments = moments.sum(axis=0).reshape(2, tok_rows)
    first = moments[0] / model_width
    second = moments[1] / model_width
    d_conv = inv_std[:, None] * (d_hat - first[:, None] - centered * second[:, None])
    padded_taps = -(-tap_count // z_size) * z_size
    sums = tap_sums(d_conv, behind, proj_value, proj_gate, tap_count, padded_taps)
    head, sums = lax.optimization_barrier((d_conv[:overhang], sums))
    ahead = passed_along(head, SP, -1)
    grad_value, grad_gate = filtered(d_conv, ahead, proj_value, proj_gate, conv_taps)
    tap_part = scattered_sum(sums, "z")
    tap_part, grad_value, grad_gate = lax.optimization_barrier((tap_part, grad_value, grad_gate))
    tap_part = taken_together(tap_part, "y")
    each = terms.shape[1]
    spread = jnp.broadcast_to(tap_part[None], (z_size, *tap_part.shape))
    arrived = lax.all_to_all(jnp.concatenate([terms, spread], axis=1), "z", 0, 0, tiled=True)
    weight_rows, grad_taps = closing(arrived, grad_scale, each, tap_count)
    grad_out_weight = weight_rows.T
    return (grad_value, grad_gate, grad_out_weight, grad_taps)


def solution(mesh):
    split = Mesh(mesh.devices.reshape(12, 8, mesh.shape["tp"]), (*SP, "tp"))
    return jax.shard_map(
        local,
        mesh=split,
        in_specs=(
            P(SP, "tp"),
            P(SP, "tp"),
            P(SP, "tp"),
            P(None, "tp"),
            P("tp"),
            P("tp", None),
            P(SP, None),
        ),
        out_specs=(P(SP, "tp"), P(SP, "tp"), P("tp", SP), P(None, "tp")),
        check_vma=False,
    )
```

```python
import functools
import math

import jax
import jax.numpy as jnp
from jax import lax
from jax.experimental import pallas as pl
from jax.experimental.pallas import tpu as pltpu
from jax.sharding import Mesh
from jax.sharding import PartitionSpec as P

SP = ("z", "y")

norm_eps = 1e-05


def from_everyone(x, axis):
    size = lax.axis_size(axis)
    return lax.all_to_all(jnp.broadcast_to(x[None], (size, *x.shape)), axis, 0, 0, tiled=True)


def taken_together(x, axis):
    return from_everyone(x, axis).sum(axis=0)


def scattered_sum(x, axes):
    size = lax.axis_size(axes)
    rows, width = x.shape
    each = -(-rows // size)
    padded = jnp.pad(x, ((0, each * size - rows), (0, 0))).reshape(size, each, width)
    return lax.all_to_all(padded, axes, 0, 0, tiled=True).sum(axis=0)


def passed_along(block, axis, distance):
    devices = range(lax.axis_size(axis))
    route = [(i - distance, i) for i in devices if i - distance in devices]
    return lax.ppermute(block, axis, route)


def column(lanes, rows):
    turned = lanes.T
    return jnp.concatenate([turned[:, r : r + 1] for r in rows], axis=0)


def spread_rows(first, second, out_ref):
    columns = [c[at : at + 128] for c in (first, second) for at in range(0, c.shape[0], 128)]
    rows = jnp.concatenate(columns, axis=1).T
    for i in range(out_ref.shape[0]):
        out_ref[i] = rows


def statistics_kernel(conv_ref, out_ref):
    conv = conv_ref[...].astype(jnp.float32)
    spread_rows(jnp.sum(conv, axis=1, keepdims=True), jnp.sum(conv * conv, axis=1, keepdims=True), out_ref)


def statistics(conv_saved, devices):
    return pl.pallas_call(
        statistics_kernel,
        out_shape=jax.ShapeDtypeStruct((devices, conv_saved.shape[0] // 64, 128), jnp.float32),
        cost_estimate=pl.CostEstimate(flops=3 * conv_saved.size, bytes_accessed=2 * conv_saved.size, transcendentals=0),
        compiler_params=pltpu.CompilerParams(vmem_limit_bytes=8 * 2**20),
        name="statistics",
    )(conv_saved)


def standardized(model_width, shared_ref, conv_ref):
    totals = jnp.sum(shared_ref[...], axis=0) / model_width
    half = totals.shape[0] // 2
    mean = column(totals, range(half))
    square = column(totals, range(half, 2 * half))
    inv_std = lax.rsqrt(square - mean * mean + norm_eps)
    return (conv_ref[...].astype(jnp.float32) - mean) * inv_std


def norm_grad_kernel(model_width, shared_ref, conv_ref, gain_ref, act_grad_ref, hat_ref, out_ref):
    centered = standardized(model_width, shared_ref, conv_ref)
    gain = gain_ref[...].astype(jnp.float32)
    normed = centered * gain
    gate_norm = jax.nn.sigmoid(normed)
    d_hat = act_grad_ref[...] * gate_norm * (1.0 + normed * (1.0 - gate_norm)) * gain
    hat_ref[...] = d_hat
    spread_rows(jnp.sum(d_hat, axis=1, keepdims=True), jnp.sum(d_hat * centered, axis=1, keepdims=True), out_ref)


def norm_grad(model_width, shared, conv_saved, gain, act_grad):
    return pl.pallas_call(
        functools.partial(norm_grad_kernel, model_width),
        out_shape=(jax.ShapeDtypeStruct(conv_saved.shape, jnp.float32), jax.ShapeDtypeStruct(shared.shape, jnp.float32)),
        cost_estimate=pl.CostEstimate(
            flops=20 * conv_saved.size, bytes_accessed=10 * conv_saved.size, transcendentals=conv_saved.size
        ),
        compiler_params=pltpu.CompilerParams(vmem_limit_bytes=8 * 2**20),
        name="norm_grad",
    )(shared, conv_saved, gain, act_grad)


def weight_grad_kernel(model_width, z_size, shared_ref, conv_ref, gain_ref, cot_ref, out_ref, act_ref):
    centered = standardized(model_width, shared_ref, conv_ref)
    normed = centered * gain_ref[...].astype(jnp.float32)
    act_ref[...] = (normed * jax.nn.sigmoid(normed)).astype(jnp.bfloat16)
    y_size = out_ref.shape[0]
    each = out_ref.shape[1] // z_size
    block = 2 * y_size * each
    for i in range(z_size // 2):
        res = jnp.dot(cot_ref[i * block : (i + 1) * block], act_ref[...], preferred_element_type=jnp.float32)
        for g in range(2):
            for y in range(y_size):
                at, to = (g * y_size + y) * each, (2 * i + g) * each
                out_ref[y, to : to + each] = res[at : at + each]


def weight_grad(shared, conv_saved, gain, cot_t, z_size, y_size):
    model_width, width = cot_t.shape[0], conv_saved.shape[1]
    return pl.pallas_call(
        functools.partial(weight_grad_kernel, model_width, z_size),
        out_shape=jax.ShapeDtypeStruct((y_size, model_width // y_size, width), jnp.float32),
        scratch_shapes=[pltpu.VMEM(conv_saved.shape, jnp.bfloat16)],
        cost_estimate=pl.CostEstimate(
            flops=2 * conv_saved.size * model_width,
            bytes_accessed=2 * cot_t.size + 4 * model_width * width,
            transcendentals=conv_saved.size,
        ),
        compiler_params=pltpu.CompilerParams(vmem_limit_bytes=16 * 2**20),
        name="weight_grad",
    )(shared, conv_saved, gain, cot_t)


STEP = 32


def widen(taps_ref, wide_ref):
    for k in range(taps_ref.shape[0]):
        wide_ref[k] = jnp.broadcast_to(taps_ref[k : k + 1].astype(jnp.float32), wide_ref.shape[1:])


def filter_rows(window, value, gate, wide_ref, tap_sums_ref):
    tap_count = wide_ref.shape[0]
    gate_proj = jax.nn.sigmoid(gate.astype(jnp.float32))
    gated = value.astype(jnp.float32) * gate_proj
    groups = (STEP // 8, 8, gated.shape[1])
    gated_groups = gated.reshape(groups)
    d_glu = jnp.zeros(groups, jnp.float32)
    for phase in range(8):
        turned = window[phase : phase + 2 * STEP - 8]
        for at in range(phase, tap_count, 8):
            k = tap_count - 1 - at
            shifted = turned[at - phase : at - phase + STEP].reshape(groups)
            d_glu += wide_ref[k] * shifted
            tap_sums_ref[k] += (gated_groups * shifted).sum(axis=0)
    d_glu = d_glu.reshape(gated.shape)
    grad_value = d_glu * gate_proj
    grad_gate = d_glu * gated * (1.0 - gate_proj)
    return grad_value.astype(jnp.bfloat16), grad_gate.astype(jnp.bfloat16)


def main_rows_kernel(conv_grad_ref, value_ref, gate_ref, taps_ref, value_out, gate_out, tap_out, wide_ref):
    tap_out[...] = jnp.zeros_like(tap_out)
    widen(taps_ref, wide_ref)

    def one(i, carry):
        at = pl.multiple_of(i * STEP, STEP)
        rows = pl.ds(at, STEP)
        value_out[rows], gate_out[rows] = filter_rows(
            conv_grad_ref[pl.ds(at, 2 * STEP)], value_ref[rows], gate_ref[rows], wide_ref, tap_out
        )
        return carry

    lax.fori_loop(0, value_ref.shape[0] // STEP - 1, one, 0)
    last = value_ref.shape[0] - STEP
    value_out[last:] = jnp.zeros((STEP, value_out.shape[1]), value_out.dtype)
    gate_out[last:] = jnp.zeros((STEP, gate_out.shape[1]), gate_out.dtype)


def last_rows_kernel(
    conv_grad_ref, ahead_ref, value_ref, gate_ref, taps_ref, value_in, gate_in, tap_in, value_out, gate_out, tap_out, sums_ref, wide_ref
):
    last = value_ref.shape[0] - STEP
    width = conv_grad_ref.shape[1]
    ahead = ahead_ref[...]
    fill = jnp.zeros((STEP - ahead.shape[0], width), jnp.float32)
    window = jnp.concatenate([conv_grad_ref[last:], ahead, fill], axis=0)
    sums_ref[...] = tap_in[...]
    widen(taps_ref, wide_ref)
    value_out[:last] = value_in[:last]
    gate_out[:last] = gate_in[:last]
    value_out[last:], gate_out[last:] = filter_rows(window, value_ref[last:], gate_ref[last:], wide_ref, sums_ref)
    tap_count = taps_ref.shape[0]
    tap_out[:tap_count] = jnp.sum(sums_ref[...], axis=1)
    tap_out[tap_count:] = jnp.zeros((tap_out.shape[0] - tap_count, width), jnp.float32)


def main_rows(conv_grad, value, gate, taps):
    grad = jax.ShapeDtypeStruct(value.shape, jnp.bfloat16)
    return pl.pallas_call(
        main_rows_kernel,
        out_shape=(grad, grad, jax.ShapeDtypeStruct((taps.shape[0], 8, taps.shape[1]), jnp.float32)),
        scratch_shapes=[pltpu.VMEM((taps.shape[0], 8, taps.shape[1]), jnp.float32)],
        cost_estimate=pl.CostEstimate(flops=4 * taps.shape[0] * value.size, bytes_accessed=12 * value.size, transcendentals=value.size),
        compiler_params=pltpu.CompilerParams(vmem_limit_bytes=12 * 2**20),
        name="main_rows",
    )(conv_grad, value, gate, taps)


def last_rows(conv_grad, ahead, value, gate, taps, done, padded_taps):
    grad = jax.ShapeDtypeStruct(value.shape, jnp.bfloat16)
    return pl.pallas_call(
        last_rows_kernel,
        out_shape=(grad, grad, jax.ShapeDtypeStruct((padded_taps, taps.shape[1]), jnp.float32)),
        scratch_shapes=[pltpu.VMEM(done[2].shape, jnp.float32)] * 2,
        cost_estimate=pl.CostEstimate(flops=4 * taps.size * STEP, bytes_accessed=16 * value.size, transcendentals=0),
        compiler_params=pltpu.CompilerParams(vmem_limit_bytes=12 * 2**20),
        name="last_rows",
    )(conv_grad, ahead, value, gate, taps, *done)


def closing_kernel(scale, arrived_ref, weight_out, tap_out):
    each = weight_out.shape[0]
    total = arrived_ref[0]
    for z in range(1, arrived_ref.shape[0]):
        total = total + arrived_ref[z]
    weight_out[...] = total[:each] * scale
    rows = arrived_ref.shape[1] - each
    for z in range(arrived_ref.shape[0]):
        at = z * rows
        count = min(rows, tap_out.shape[0] - at)
        if count > 0:
            tap_out[at : at + count] = arrived_ref[z, each : each + count] * scale


def closing(arrived, scale, each, tap_count):
    width = arrived.shape[2]
    return pl.pallas_call(
        functools.partial(closing_kernel, scale),
        out_shape=(jax.ShapeDtypeStruct((each, width), jnp.float32), jax.ShapeDtypeStruct((tap_count, width), jnp.float32)),
        cost_estimate=pl.CostEstimate(flops=arrived.size, bytes_accessed=4 * arrived.size, transcendentals=0),
        compiler_params=pltpu.CompilerParams(vmem_limit_bytes=4 * 2**20),
        name="closing",
    )(arrived)


def local(proj_value, proj_gate, conv_saved, conv_taps, norm_gain, out_weight, cotangent):
    model_width = cotangent.shape[1]
    tok_rows = cotangent.shape[0]
    tap_count = conv_taps.shape[0]
    overhang = tap_count - 1
    grad_scale = 1.0 / math.sqrt(tok_rows * lax.axis_size(SP))
    z_size, y_size = (lax.axis_size(a) for a in SP)
    d_act = lax.dot_general(
        cotangent, out_weight, (((1,), (1,)), ((), ())), preferred_element_type=jnp.float32
    )
    everyone = lambda x: lax.all_to_all(x, "tp", 0, 0, tiled=True)
    shared = everyone(statistics(conv_saved, lax.axis_size("tp")))
    shared, d_act = lax.optimization_barrier((shared, d_act))
    terms = weight_grad(shared, conv_saved, norm_gain[None], cotangent.T, z_size, y_size)
    terms = lax.psum_scatter(terms, "y", scatter_dimension=0)
    terms = terms.reshape(z_size, -1, terms.shape[1])
    d_hat, moments = norm_grad(model_width, shared, conv_saved, norm_gain[None], d_act)
    moments = everyone(moments)
    totals = shared.sum(axis=0).reshape(2, tok_rows)
    row_mean = totals[0] / model_width
    row_var = totals[1] / model_width - row_mean * row_mean
    inv_std = lax.rsqrt(row_var + norm_eps)
    centered = (conv_saved.astype(jnp.float32) - row_mean[:, None]) * inv_std[:, None]
    moments = moments.sum(axis=0).reshape(2, tok_rows)
    first = moments[0] / model_width
    second = moments[1] / model_width
    d_conv = inv_std[:, None] * (d_hat - first[:, None] - centered * second[:, None])
    ahead = passed_along(d_conv[:overhang], SP, -1)
    done = main_rows(d_conv, proj_value, proj_gate, conv_taps)
    padded_taps = -(-tap_count // z_size) * z_size
    grad_value, grad_gate, tap_sums = last_rows(d_conv, ahead, proj_value, proj_gate, conv_taps, done, padded_taps)
    tap_part = taken_together(scattered_sum(tap_sums, "z"), "y")
    each = terms.shape[1]
    spread = jnp.broadcast_to(tap_part[None], (z_size, *tap_part.shape))
    arrived = lax.all_to_all(jnp.concatenate([terms, spread], axis=1), "z", 0, 0, tiled=True)
    weight_rows, grad_taps = closing(arrived, grad_scale, each, tap_count)
    grad_out_weight = weight_rows.T
    return (grad_value, grad_gate, grad_out_weight, grad_taps)


def solution(mesh):
    split = Mesh(mesh.devices.reshape(12, 8, mesh.shape["tp"]), (*SP, "tp"))
    return jax.shard_map(
        local,
        mesh=split,
        in_specs=(
            P(SP, "tp"),
            P(SP, "tp"),
            P(SP, "tp"),
            P(None, "tp"),
            P("tp"),
            P("tp", None),
            P(SP, None),
        ),
        out_specs=(P(SP, "tp"), P(SP, "tp"), P("tp", SP), P(None, "tp")),
        check_vma=False,
    )
```
